32 devices in a mesh: fs: 8 (over z, x), tp: 4 (over y, core).
Axes of the slice: x: 2, y: 2, z: 4, core: 2. Of those that a mesh axis runs over, the one named last changes fastest.
Arguments:
- seq_rows: bfloat16 [6144, 2048], P('fs', 'tp'), may hold values from -6 to 6
- mixer_gain: bfloat16 [2048], P('tp'), may hold values from 0.099609375 to 1.8984375
- query_weight: bfloat16 [2048, 2048], P('fs', 'tp'), may hold values from -0.125 to 0.125
- key_weight: bfloat16 [2048, 2048], P('fs', 'tp'), may hold values from -0.125 to 0.125
- value_weight: bfloat16 [2048, 4096], P('fs', 'tp'), may hold values from -0.125 to 0.125
- decay_logs: float32 [8], P('tp'), may hold values from -0.0333333333 to -0.000390625
- mixer_out_weight: bfloat16 [4096, 2048], P('tp', 'fs'), may hold values from -0.125 to 0.125
- channel_gain: bfloat16 [2048], P('tp'), may hold values from 0.099609375 to 1.8984375
- value_up_weight: bfloat16 [2048, 5632], P('fs', 'tp'), may hold values from -0.125 to 0.125
- gate_up_weight: bfloat16 [2048, 5632], P('fs', 'tp'), may hold values from -0.125 to 0.125
- conv_taps: bfloat16 [3, 5632], P(None, 'tp'), may hold values from -3 to 3
- conv_bias: bfloat16 [5632], P('tp'), may hold values from -3 to 3
- down_weight: bfloat16 [5632, 2048], P('tp', 'fs'), may hold values from -0.109375 to 0.109375
Outputs:
- layer_out: bfloat16 [6144, 2048], P('fs', 'tp')
The draws below stay inside these ranges and needn't reach their ends.
All inputs are finite; a program needn't handle non-finite values.
Results may differ from the reference program's by a relative error of at most 0.02.
Values may be sent and summed in bfloat16 or wider, within the bound.
A program may use at most 128 MiB of HBM per device.

```python
import jax
import jax.numpy as jnp
from jax import lax

D = 2048
HEADS = 8
DK = 256
DV = 512
FF = 5632
KW = 3
BLOCK = 128
SEQ_LEN = 768
TOKENS = 6144
N_TP = 4


def draw_decay_logs(key, part):
    pick_key = jax.random.fold_in(key, 11)
    fast_key = jax.random.fold_in(key, 12)
    slow_key = jax.random.fold_in(key, 13)
    order = jax.random.permutation(pick_key, HEADS)
    quick = order < HEADS // 2
    fast = -1.0 / jax.random.uniform(fast_key, (HEADS,), jnp.float32, 30.0, 100.0)
    slow = -jax.random.uniform(slow_key, (HEADS,), jnp.float32, 0.3, 2.0) / SEQ_LEN
    return jnp.where(quick, fast, slow).astype(jnp.float32)


def strengthened(array, own_key, source, target, blocks, factor):
    def block_of(dim):
        return (jnp.arange(array.shape[dim]) // (array.shape[dim] // blocks)).reshape((-1,) + (1,) * (array.ndim - 1 - dim))

    one_side = jax.random.permutation(own_key, blocks)[block_of(target)]
    far = (block_of(target) + blocks // 2) % blocks
    return jnp.where((block_of(source) == one_side) | (block_of(source) == far), factor * array, array)


def levels(key, shape, split, least, high):
    level, own = 1.0, jax.random.fold_in(key, 6)
    for dim, parts in split:
        heights = jnp.exp(jax.random.uniform(jax.random.fold_in(own, dim), (parts,), jnp.float32, least / len(split), high / len(split)))
        level = level * jnp.repeat(heights, shape[dim] // parts).reshape([-1 if axis == dim else 1 for axis in range(len(shape))])
    return level


def scatter_about(rng, shape, scale, most, pieces=(), kind=jnp.bfloat16):
    gain = levels(rng, shape, pieces, -0.22, 0.18) if pieces else 1.0
    values = jax.random.normal(rng, shape, jnp.float32) * scale * gain
    return jnp.minimum(jnp.maximum(values, -most), most).astype(kind)


def noise_with(own_key, dims, scale, limit, split, heavy, kind=jnp.bfloat16):
    drawn = scale * jax.random.normal(own_key, dims, jnp.float32)
    if split:
        drawn = drawn * levels(own_key, dims, split, -0.22, 0.18)
    return jnp.clip(strengthened(drawn, jax.random.fold_in(own_key, 3), *heavy), -limit, limit).astype(kind)


def setup_inputs(seed: int = 0) -> dict:
    keys = jax.random.split(jax.random.key(seed), 14)
    seq_rows = scatter_about(keys[0], (TOKENS, D), 1.0, 6.0, ((0, 8), (1, 4)))
    mixer_gain = jnp.clip(1.0 + 0.18 * jax.random.normal(keys[1], (D,), jnp.float32), 0.099609375, 1.8984375).astype(jnp.bfloat16)
    query_weight = scatter_about(keys[2], (D, HEADS * DK), D ** -0.5, 0.125, ((0, 8), (1, 4)))
    key_weight = scatter_about(keys[3], (D, HEADS * DK), D ** -0.5, 0.125, ((0, 8), (1, 4)))
    value_weight = scatter_about(keys[4], (D, HEADS * DV), D ** -0.5, 0.125, ((0, 8), (1, 4)))
    decay_logs = draw_decay_logs(jax.random.fold_in(keys[13], 71), 0)
    mixer_out_weight = noise_with(keys[6], (HEADS * DV, D), (HEADS * DV) ** -0.5, 0.125, ((0, 4), (1, 8)), (0, 1, 8, 2.0))
    channel_gain = jnp.clip(1.0 + 0.18 * jax.random.normal(keys[7], (D,), jnp.float32), 0.099609375, 1.8984375).astype(jnp.bfloat16)
    value_up_weight = scatter_about(keys[8], (D, FF), D ** -0.5, 0.125, ((0, 8), (1, 4)))
    gate_up_weight = scatter_about(keys[9], (D, FF), D ** -0.5, 0.125, ((0, 8), (1, 4)))
    conv_taps = scatter_about(keys[10], (KW, FF), 0.6, 3.0, ((1, 4),))
    conv_bias = scatter_about(keys[11], (FF,), 0.5, 3.0, ((0, 4),))
    down_weight = noise_with(keys[12], (FF, D), FF ** -0.5, 0.109375, ((0, 4), (1, 8)), (0, 1, 8, 2.0))
    return dict(seq_rows=seq_rows, mixer_gain=mixer_gain, query_weight=query_weight, key_weight=key_weight, value_weight=value_weight, decay_logs=decay_logs, mixer_out_weight=mixer_out_weight, channel_gain=channel_gain, value_up_weight=value_up_weight, gate_up_weight=gate_up_weight, conv_taps=conv_taps, conv_bias=conv_bias, down_weight=down_weight)


EPS = 1e-06
ROPE_BASE = 10000.0
HIGH_PRECISION = lax.Precision.HIGHEST

def rotate_heads(tensor, cosine, sine):
    half = tensor.shape[-1] // 2
    first = tensor[..., :half]
    second = tensor[..., half:]
    return jnp.concatenate([first * cosine - second * sine, first * sine + second * cosine], axis=-1)

def retention_blocks(query, key, value, decay_logs):
    length, heads = (query.shape[0], query.shape[1])
    count = length // BLOCK
    offsets = jnp.arange(BLOCK, dtype=jnp.float32)
    spread = offsets[:, None] - offsets[None, :]
    within_block = jnp.where(spread[None] >= 0.0, jnp.exp(decay_logs[:, None, None] * jnp.maximum(spread, 0.0)[None]), 0.0)
    carried = jnp.exp(decay_logs[:, None] * (offsets + 1.0))
    state_decay_factor = jnp.exp(decay_logs[:, None] * (BLOCK - 1.0 - offsets))
    block_decay_factor = jnp.exp(decay_logs * BLOCK)

    def blocks(tensor):
        return tensor.reshape(count, BLOCK, heads, tensor.shape[-1]).transpose(0, 2, 1, 3)

    def advance(recurrent_state, triple):
        query_block, key_block, value_block = triple
        attention_scores = jnp.einsum('ucf,uxf->ucx', query_block, key_block, precision=HIGH_PRECISION) * within_block
        result = jnp.einsum('hnm,hmv->hnv', attention_scores, value_block, precision=HIGH_PRECISION)
        result = result + jnp.einsum('hnd,hdv->hnv', query_block, recurrent_state, precision=HIGH_PRECISION) * carried[:, :, None]
        recurrent_state = block_decay_factor[:, None, None] * recurrent_state + jnp.einsum('ieb,iez->ibz', key_block * state_decay_factor[:, :, None], value_block, precision=HIGH_PRECISION)
        return (recurrent_state, result)
    start = jnp.zeros((heads, query.shape[-1], value.shape[-1]), jnp.float32)
    _, result = lax.scan(advance, start, (blocks(query), blocks(key), blocks(value)))
    return result.transpose(0, 2, 1, 3).reshape(length, heads, value.shape[-1])

def grouped_sum(left, right, groups):
    width = left.shape[1] // groups

    def add_group(index, total):
        begin = (index * width).astype(jnp.int32)
        term = jnp.dot(lax.dynamic_slice_in_dim(left, begin, width, 1), lax.dynamic_slice_in_dim(right, begin, width, 0), preferred_element_type=jnp.float32)
        rounded = lax.optimization_barrier(term.astype(jnp.bfloat16))
        return total + rounded.astype(jnp.float32)
    start = jnp.zeros((left.shape[0], right.shape[1]), jnp.float32)
    return lax.fori_loop(jnp.int32(0), jnp.int32(groups), add_group, start)

def one_sequence(rows, mixer_gain, query_weight, key_weight, value_weight, decay_logs, mixer_out_weight, channel_gain, value_up_weight, gate_up_weight, conv_taps, conv_bias, down_weight):
    length = rows.shape[0]
    rows_f = rows.astype(jnp.float32)
    scale_one = lax.rsqrt(lax.optimization_barrier(jnp.mean(rows_f * rows_f, axis=-1, keepdims=True)) + EPS)
    scaled_one = (rows_f * mixer_gain.astype(jnp.float32)).astype(jnp.bfloat16)
    query = (jnp.dot(scaled_one, query_weight, preferred_element_type=jnp.float32) * scale_one).astype(jnp.bfloat16)
    key = (jnp.dot(scaled_one, key_weight, preferred_element_type=jnp.float32) * scale_one).astype(jnp.bfloat16)
    value = (jnp.dot(scaled_one, value_weight, preferred_element_type=jnp.float32) * scale_one).astype(jnp.bfloat16)
    half = DK // 2
    freqs = jnp.power(ROPE_BASE, -jnp.arange(half, dtype=jnp.float32) * 2.0 / DK)
    angles = jnp.arange(length, dtype=jnp.float32)[:, None] * freqs[None, :]
    cosine = jnp.cos(angles)[:, None, :]
    sine = jnp.sin(angles)[:, None, :]
    turned_q = rotate_heads(query.astype(jnp.float32).reshape(length, HEADS, DK), cosine, sine)
    turned_k = rotate_heads(key.astype(jnp.float32).reshape(length, HEADS, DK), cosine, sine) * DK ** (-0.5)
    ret = retention_blocks(turned_q, turned_k, value.astype(jnp.float32).reshape(length, HEADS, DV), decay_logs)
    centred = ret - lax.optimization_barrier(jnp.mean(ret, axis=-1, keepdims=True))
    normed = (centred * lax.rsqrt(lax.optimization_barrier(jnp.mean(centred * centred, axis=-1, keepdims=True)) + EPS)).reshape(length, HEADS * DV).astype(jnp.bfloat16)
    mixed = grouped_sum(normed, mixer_out_weight, N_TP)
    middle = (rows_f + mixed).astype(jnp.bfloat16)
    middle_f = middle.astype(jnp.float32)
    scale_two = lax.rsqrt(lax.optimization_barrier(jnp.mean(middle_f * middle_f, axis=-1, keepdims=True)) + EPS)
    scaled_two = (middle_f * channel_gain.astype(jnp.float32)).astype(jnp.bfloat16)
    up_val = (jnp.dot(scaled_two, value_up_weight, preferred_element_type=jnp.float32) * scale_two).astype(jnp.bfloat16)
    up_gate = (jnp.dot(scaled_two, gate_up_weight, preferred_element_type=jnp.float32) * scale_two).astype(jnp.bfloat16)
    padded = jnp.concatenate([jnp.zeros((KW - 1, FF), jnp.float32), up_gate.astype(jnp.float32)], axis=0)
    conv = jnp.zeros((length, FF), jnp.float32) + conv_bias.astype(jnp.float32)[None, :]
    for tap in range(KW):
        conv = conv + conv_taps[tap].astype(jnp.float32)[None, :] * padded[tap:tap + length]
    hidden = (jax.nn.silu(conv) * up_val.astype(jnp.float32)).astype(jnp.bfloat16)
    channel = grouped_sum(hidden, down_weight, N_TP)
    return (middle_f + channel).astype(jnp.bfloat16)

def reference(seq_rows, mixer_gain, query_weight, key_weight, value_weight, decay_logs, mixer_out_weight, channel_gain, value_up_weight, gate_up_weight, conv_taps, conv_bias, down_weight):
    sequences = seq_rows.reshape(TOKENS // SEQ_LEN, SEQ_LEN, D)

    def run(rows):
        return one_sequence(rows, mixer_gain, query_weight, key_weight, value_weight, decay_logs, mixer_out_weight, channel_gain, value_up_weight, gate_up_weight, conv_taps, conv_bias, down_weight)
    return lax.map(run, sequences).reshape(TOKENS, D)
```

```python
import functools

import jax
import jax.numpy as jnp
import numpy as np
from jax import lax
from jax.experimental import pallas as pl
from jax.experimental.pallas import tpu as pltpu
from jax.sharding import PartitionSpec as P

DK = 256
DV = 512
KW = 3
EPS = 1e-06
ROPE_BASE = 10000.0
LANES = 128
ROWS = 256
PAD = 8
BF16 = jnp.bfloat16
F32 = jnp.float32


def flip(index, mask):
    return index + mask * (1 - 2 * lax.rem(lax.div(index, mask), 2))


def flips(index, mask):
    bit = 1
    while bit <= mask:
        if mask & bit:
            index = flip(index, bit)
        bit *= 2
    return index


def bits_of(size):
    return [1 << i for i in range(size.bit_length() - 1)]


class Plan:
    def __init__(self, fs, tp, length, block, heads_here, ff_here, shard):
        self.fs, self.tp, self.length, self.block, self.shard = fs, tp, length, block, shard
        self.width = fs * shard
        self.paired = heads_here % 2 == 0 and ff_here % LANES == 0 and fs >= 4
        self.heads = heads_here // 2 if self.paired else heads_here
        self.ff = -(-ff_here // (2 * LANES)) * LANES if self.paired else ff_here
        self.ff_step = ff_here - self.ff
        self.seqs = 2 if self.paired else 1
        self.rows = self.seqs * length
        self.pair = 2 if self.paired else 0
        self.gather = ([self.pair] if self.paired else []) + [b for b in bits_of(fs)[::-1] if b != self.pair]
        self.dims = [("tp", b) for b in bits_of(tp)] + ([("fs", self.pair)] if self.paired else [])
        self.qk = self.heads * DK
        self.dv = self.heads * DV
        self.heads_step = self.heads


class Mail:
    def __init__(self, sends, recvs, me):
        self.sends, self.recvs, self.me = sends, recvs, me
        self.count = 0
        self.ids = {}
        self.sent = []

    def id_of(self, key):
        if key not in self.ids:
            self.ids[key] = len(self.ids)
        return self.ids[key]

    def copy(self, key, src, dst, axis, mask):
        n = self.id_of(key)
        return pltpu.make_async_remote_copy(
            src_ref=src,
            dst_ref=dst,
            send_sem=self.sends.at[n],
            recv_sem=self.recvs.at[n],
            device_id={axis: flip(self.me[axis], mask)},
            device_id_type=pl.DeviceIdType.MESH,
        )

    def send(self, key, src, dst, axis, mask):
        copy = self.copy(key, src, dst, axis, mask)
        copy.start()
        self.sent.append(copy)
        return copy

    def arrive(self, key, slot, axis, mask):
        self.copy(key, slot, slot, axis, mask).wait_recv()

    def drain(self):
        for copy in self.sent:
            copy.wait_send()
        self.sent = []


class Stream:
    def __init__(self, plan, mail, name, slot, stage):
        self.plan, self.mail, self.name, self.slot, self.stage = plan, mail, name, slot, stage
        self.mine = mail.me["fs"]
        self.bits = plan.gather

    def at(self, code):
        return self.slot(flips(self.mine, code))

    def forward(self, code, first):
        for bit in self.bits[first:]:
            src = self.stage if bit == self.plan.pair else self.at(code)
            self.mail.send((self.name, bit, code), src, self.at(code), "fs", bit)

    def begin(self):
        self.forward(0, 0)
        self.todo = []
        codes = [0]
        for place, bit in enumerate(self.bits):
            new = [c | bit for c in codes]
            self.todo += [(c, bit, place) for c in new]
            codes = codes + new

    def step(self, times=1):
        for _ in range(times):
            if self.todo:
                code, bit, place = self.todo.pop(0)
                self.mail.arrive((self.name, bit, code & ~bit), self.at(code), "fs", bit)
                self.forward(code, place + 1)

    def steps_left(self):
        return sum(1 for t in self.todo if t[2] < len(self.bits) - 1)

    def finish(self):
        self.step(len(self.todo))


def kernel(
    plan,
    x_hbm, gain_hbm, cos_hbm, sin_hbm, q_hbm, k_hbm, v_hbm, decay, out_hbm, val_hbm, gate_hbm, conv_hbm, down_hbm,
    result,
    w_in, w_out, w_val, w_gate, w_down, s_in, s_out, s_val, s_gate, s_down,
    act, act2, gains, cosine, sine, conv_par, qk, value, normed, part, hidden, gates,
    *rest,
):
    n_dims = len(plan.dims)
    recvs, outs = rest[:n_dims], rest[n_dims : 2 * n_dims - 1]
    sends, arrivals, local = rest[2 * n_dims - 1 :]
    me = {"fs": lax.axis_index("fs"), "tp": lax.axis_index("tp")}
    length, block, shard = plan.length, plan.block, plan.shard
    row_blocks = length // ROWS
    seq = lax.rem(lax.div(me["fs"], plan.pair), 2) if plan.paired else 0

    barrier = pltpu.get_barrier_semaphore()
    near = [("fs", b) for b in plan.gather] + [d for d in plan.dims if d[0] == "tp"]
    for axis, bit in near:
        pl.semaphore_signal(
            barrier, inc=1, device_id={axis: flip(me[axis], bit)}, device_id_type=pl.DeviceIdType.MESH
        )

    places = []

    def fetch(src, dst):
        copy = pltpu.make_async_copy(src, dst, local.at[len(places)])
        copy.start()
        places.append(copy)

    def columns(index, width, size=None):
        return pl.ds(pl.multiple_of(index * width, width), size or width)

    def own_block(ref, s, t):
        return ref.at[columns(s, length), columns(t, block)]

    fetch(x_hbm, own_block(act, seq, me["tp"]))
    fetch(gain_hbm, gains.at[:, columns(me["tp"], block)])
    mine = me["fs"]
    rows_in = columns(mine, shard)

    def halves(dst, stage, take):
        fetch(take(seq), dst)
        if plan.paired:
            fetch(take(1 - seq), stage)

    qk_w, dv_w = plan.qk, plan.dv
    halves(w_in.at[rows_in, 0:qk_w], s_in.at[:, 0:qk_w], lambda h: q_hbm.at[:, columns(h, qk_w)])
    halves(
        w_in.at[rows_in, qk_w : 2 * qk_w], s_in.at[:, qk_w : 2 * qk_w], lambda h: k_hbm.at[:, columns(h, qk_w)]
    )
    halves(
        w_in.at[rows_in, 2 * qk_w : 2 * qk_w + dv_w],
        s_in.at[:, 2 * qk_w : 2 * qk_w + dv_w],
        lambda h: v_hbm.at[:, columns(h, dv_w)],
    )
    n_first = len(places)
    halves(w_out.at[:, columns(mine, shard)], s_out, lambda h: out_hbm.at[columns(h, dv_w), :])

    def ff_part(h):
        if not plan.paired:
            return slice(None)
        return pl.ds(pl.multiple_of(h * plan.ff_step, LANES), plan.ff)

    halves(w_val.at[rows_in, :], s_val, lambda h: val_hbm.at[:, ff_part(h)])
    halves(w_gate.at[rows_in, :], s_gate, lambda h: gate_hbm.at[:, ff_part(h)])
    halves(w_down.at[:, columns(mine, shard)], s_down, lambda h: down_hbm.at[ff_part(h), :])
    fetch(cos_hbm, cosine)
    fetch(sin_hbm, sine)
    fetch(conv_hbm.at[:, ff_part(seq)], conv_par)

    mail = Mail(sends, arrivals, me)
    st_in = Stream(plan, mail, "in", lambda j: w_in.at[columns(j, shard), :], s_in)
    st_out = Stream(plan, mail, "out", lambda j: w_out.at[:, columns(j, shard)], s_out)
    st_val = Stream(plan, mail, "val", lambda j: w_val.at[columns(j, shard), :], s_val)
    st_gate = Stream(plan, mail, "gate", lambda j: w_gate.at[columns(j, shard), :], s_gate)
    st_down = Stream(plan, mail, "down", lambda j: w_down.at[:, columns(j, shard)], s_down)

    def seq_of(code):
        return 1 - seq if plan.paired and code >> (n_dims - 1) else seq

    def tp_of(code):
        return flips(me["tp"], code & (plan.tp - 1))

    class Gather:
        def __init__(self, name, at, dims):
            self.name, self.at, self.dims = name, at, dims
            self.todo = []

        def forward(self, code, last):
            for place in range(last - 1, -1, -1):
                axis, bit = self.dims[place]
                mail.send((self.name, place, code), self.at(code), self.at(code), axis, bit)

        def begin(self):
            self.forward(0, len(self.dims))
            codes = [0]
            for place in range(len(self.dims) - 1, -1, -1):
                new = [c | (1 << place) for c in codes]
                self.todo += [(c, place) for c in new]
                codes = codes + new

        def step(self, times):
            for _ in range(times):
                code, place = self.todo.pop(0)
                axis, bit = self.dims[place]
                mail.arrive((self.name, place, code & ~(1 << place)), self.at(code), axis, bit)
                self.forward(code, place)

        def finish(self):
            self.step(len(self.todo))

    tp_dims = [d for d in plan.dims if d[0] == "tp"]
    gather_gain = Gather("gain", lambda c: gains.at[:, columns(tp_of(c), block)], tp_dims)
    gather_one = Gather("one", lambda c: own_block(act, seq_of(c), tp_of(c)), plan.dims)
    gather_two = Gather("two", lambda c: own_block(act2, seq_of(c), tp_of(c)), plan.dims)

    for copy in places[:n_first]:
        copy.wait()
    pl.semaphore_wait(barrier, len(near))
    gather_one.begin()
    gather_gain.begin()
    st_in.begin()
    for copy in places[n_first:]:
        copy.wait()
    gather_one.step(1)
    st_in.step(1)
    st_out.begin()
    gather_one.step(2)
    gather_gain.step(1)
    st_in.step(1)
    st_val.begin()
    st_in.step(1)
    st_out.step(1)
    gather_one.finish()
    gather_gain.finish()
    st_out.step(1)
    st_gate.begin()
    st_in.finish()

    def scaled_rows(ref, start, gain_row):
        rows_f = ref[pl.ds(start, ROWS), :].astype(F32)
        factor = lax.rsqrt(jnp.mean(rows_f * rows_f, axis=-1, keepdims=True) + EPS)
        gain = gains[gain_row : gain_row + 1, :].astype(F32)
        return (rows_f * gain).astype(BF16), factor

    def project(i, _):
        start = pl.multiple_of(i * ROWS, ROWS)
        spot = pl.ds(pl.multiple_of(lax.rem(i, row_blocks) * ROWS, ROWS), ROWS)
        scaled, factor = scaled_rows(act, start, 0)
        total = jnp.dot(scaled, w_in[...], preferred_element_type=F32)
        cos, sin = cosine[spot, :], sine[spot, :]
        half = DK // 2
        for which, scale in ((0, 1.0), (1, DK**-0.5)):
            for head in range(plan.heads):
                at = which * qk_w + head * DK
                turned = (total[:, at : at + DK] * factor).astype(BF16).astype(F32)
                one, two = turned[:, :half], turned[:, half:]
                qk[pl.ds(start, ROWS), at : at + half] = ((one * cos - two * sin) * scale).astype(BF16)
                qk[pl.ds(start, ROWS), at + half : at + DK] = ((one * sin + two * cos) * scale).astype(BF16)
        value[pl.ds(start, ROWS), :] = (total[:, 2 * qk_w :] * factor).astype(BF16)
        return 0

    lax.fori_loop(0, plan.rows // ROWS, project, 0)
    st_out.step(1)
    st_val.step(1)

    def retain(s, _):
        for head in range(plan.heads):
            log_decay = decay[seq * plan.heads + head]
            for b in range(row_blocks):
                seen = (b + 1) * ROWS
                first = pl.multiple_of(s * length, ROWS)
                rows = pl.ds(pl.multiple_of(first + b * ROWS, ROWS), ROWS)
                keys = pl.ds(first, seen)
                query = qk[rows, head * DK : (head + 1) * DK]
                key = qk[keys, qk_w + head * DK : qk_w + (head + 1) * DK]
                scores = lax.dot_general(query, key, (((1,), (1,)), ((), ())), preferred_element_type=F32)
                spread = (
                    lax.broadcasted_iota(jnp.int32, (ROWS, seen), 0)
                    - lax.broadcasted_iota(jnp.int32, (ROWS, seen), 1)
                    + b * ROWS
                )
                fall = jnp.exp(log_decay * jnp.maximum(spread, 0).astype(F32))
                scores = jnp.where(spread >= 0, scores * fall, 0.0).astype(BF16)
                ret = jnp.dot(scores, value[keys, head * DV : (head + 1) * DV], preferred_element_type=F32)
                centred = ret - jnp.mean(ret, axis=-1, keepdims=True)
                scale = lax.rsqrt(jnp.mean(centred * centred, axis=-1, keepdims=True) + EPS)
                normed[rows, head * DV : (head + 1) * DV] = (centred * scale).astype(BF16)
        return 0

    lax.fori_loop(0, plan.seqs, retain, 0)
    st_out.finish()

    n_codes = 1 << n_dims

    def block_rows(s, i):
        return pl.ds(pl.multiple_of(s * length + i * ROWS, ROWS), ROWS)

    def multiply(left, right, code):
        cols = columns(tp_of(code), block)
        s = seq_of(code)

        def body(i, _):
            rows = block_rows(s, i)
            part[rows, cols] = jnp.dot(left[rows, :], right[:, cols], preferred_element_type=F32).astype(BF16)
            return 0

        lax.fori_loop(0, row_blocks, body, 0)

    def low(code):
        return next(i for i in range(n_dims) if code >> i & 1) if code else n_dims

    def summed(code, i):
        rows = pl.ds(pl.multiple_of(i * ROWS, ROWS), ROWS)
        total = part[block_rows(seq_of(code), i), columns(tp_of(code), block)].astype(F32)
        for place in range(low(code)):
            total = total + recvs[place][code >> (place + 1), rows, :].astype(F32)
        return total

    def scatter(name, left, right, write, between):
        order = sorted(range(n_codes), key=lambda c: (low(c) > 0, -c))
        sent = []

        def ship(code, src):
            place = low(code)
            axis, bit = plan.dims[place]
            sent.append(mail.send((name, place, code), src, recvs[place].at[code >> (place + 1)], axis, bit))

        for code in order:
            multiply(left, right, code)
            if code & 1:
                ship(code, own_block(part, seq_of(code), tp_of(code)))
        for place in range(1, n_dims + 1):
            codes = [c for c in range(n_codes) if low(c) == place][::-1]
            for code in codes:
                for k in range(place):
                    axis, bit = plan.dims[k]
                    key = (name, k, code | (1 << k))
                    if key not in waited:
                        waited.add(key)
                        mail.arrive(key, recvs[k].at[code >> (k + 1)], axis, bit)
                if place < n_dims:
                    target = outs[place - 1].at[code >> (place + 1)]

                    def body(i, _):
                        rows = pl.ds(pl.multiple_of(i * ROWS, ROWS), ROWS)
                        target[rows, :] = summed(code, i).astype(BF16)
                        return 0

                    lax.fori_loop(0, row_blocks, body, 0)
                    ship(code, target)
                between()

        def body(i, _):
            write(i, summed(0, i))
            return 0

        lax.fori_loop(0, row_blocks, body, 0)
        for copy in sent:
            copy.wait_send()
        mail.sent = [c for c in mail.sent if not any(c is d for d in sent)]

    waited = set()
    queue = [st_val, st_gate]

    def pump():
        for stream in queue:
            if stream.steps_left():
                stream.step(1)
                return

    def write_middle(i, total):
        rows = pl.ds(pl.multiple_of(i * ROWS, ROWS), ROWS)
        cols = columns(me["tp"], block)
        mine_rows = block_rows(seq, i)
        act2[mine_rows, cols] = (act[mine_rows, cols].astype(F32) + total).astype(BF16)

    scatter("mixed", normed, w_out, write_middle, pump)
    gather_two.begin()
    st_down.begin()
    gather_two.step(1)
    pump()
    gather_two.step(2)
    pump()
    gather_two.finish()
    while st_gate.steps_left():
        pump()
    st_val.finish()
    st_gate.finish()
    st_down.step(1)

    gates[0:PAD, :] = jnp.zeros((PAD, plan.ff), F32)
    column = lax.broadcasted_iota(jnp.int32, (1, plan.ff), 1)
    keep = column >= seq * (plan.ff - plan.ff_step) if plan.paired else None

    def expand(i, _):
        start = pl.multiple_of(i * ROWS, ROWS)
        scaled, factor = scaled_rows(act2, start, 1)
        gate = (jnp.dot(scaled, w_gate[...], preferred_element_type=F32) * factor).astype(BF16).astype(F32)
        before = gates[ROWS : ROWS + PAD, :]
        gates[0:PAD, :] = jnp.where(lax.rem(i, row_blocks) == 0, jnp.zeros_like(before), before)
        gates[PAD : PAD + ROWS, :] = gate
        conv = conv_par[KW : KW + 1, :] + jnp.zeros((ROWS, plan.ff), F32)
        for tap in range(KW):
            at = PAD - KW + 1 + tap
            conv = conv + conv_par[tap : tap + 1, :] * gates[at : at + ROWS, :]
        up = (jnp.dot(scaled, w_val[...], preferred_element_type=F32) * factor).astype(BF16).astype(F32)
        made = conv / (1.0 + jnp.exp(-conv)) * up
        if keep is not None:
            made = jnp.where(keep, made, 0.0)
        hidden[pl.ds(start, ROWS), :] = made.astype(BF16)
        return 0

    lax.fori_loop(0, plan.rows // ROWS, expand, 0)
    st_down.finish()

    def write_result(i, total):
        rows = pl.ds(pl.multiple_of(i * ROWS, ROWS), ROWS)
        cols = columns(me["tp"], block)
        result[rows, :] = (act2[block_rows(seq, i), cols].astype(F32) + total).astype(BF16)

    scatter("channel", hidden, w_down, write_result, lambda: None)
    mail.drain()


def on_device(
    seq_rows, mixer_gain, query_weight, key_weight, value_weight, decay_logs, mixer_out_weight, channel_gain,
    value_up_weight, gate_up_weight, conv_taps, conv_bias, down_weight,
):
    length, block = seq_rows.shape
    plan = Plan(
        lax.axis_size("fs"), lax.axis_size("tp"), length, block,
        query_weight.shape[1] // DK, value_up_weight.shape[1], query_weight.shape[0],
    )
    gains = jnp.concatenate(
        [mixer_gain[None], channel_gain[None], jnp.zeros((14, block), BF16)], axis=0
    )
    conv = jnp.concatenate(
        [conv_taps, conv_bias[None], jnp.zeros((PAD - KW - 1, conv_bias.shape[0]), BF16)], axis=0
    ).astype(F32)
    freqs = np.power(np.float32(ROPE_BASE), -np.arange(DK // 2, dtype=np.float32) * np.float32(2.0) / np.float32(DK))
    angles = np.arange(length, dtype=np.float32)[:, None] * freqs[None, :].astype(np.float32)
    cosine = jnp.asarray(np.cos(angles).astype(np.float32))
    sine = jnp.asarray(np.sin(angles).astype(np.float32))
    n_dims = len(plan.dims)
    rows, ff, width, shard = plan.rows, plan.ff, plan.width, plan.shard
    made = 2 * plan.qk + plan.dv
    vm = pltpu.VMEM
    n_mail = 5 * (plan.fs - 1) + 2 * ((1 << n_dims) - 1) * 2 + plan.tp
    scratch = [
        vm((width, made), BF16), vm((plan.dv, width), BF16), vm((width, ff), BF16), vm((width, ff), BF16),
        vm((ff, width), BF16),
        vm((shard, made), BF16), vm((plan.dv, shard), BF16), vm((shard, ff), BF16), vm((shard, ff), BF16),
        vm((ff, shard), BF16),
        vm((rows, width), BF16), vm((rows, width), BF16), vm((16, width), BF16),
        vm((length, DK // 2), F32), vm((length, DK // 2), F32), vm((PAD, ff), F32),
        vm((rows, 2 * plan.qk), BF16), vm((rows, plan.dv), BF16), vm((rows, plan.dv), BF16),
        vm((rows, width), BF16), vm((rows, ff), BF16), vm((ROWS + PAD, ff), F32),
    ]
    scratch += [vm((1 << (n_dims - 1 - k), length, block), BF16) for k in range(n_dims)]
    scratch += [vm((1 << (n_dims - 1 - k), length, block), BF16) for k in range(1, n_dims)]
    scratch += [
        pltpu.SemaphoreType.DMA((n_mail,)), pltpu.SemaphoreType.DMA((n_mail,)), pltpu.SemaphoreType.DMA((24,)),
    ]
    hbm = pl.BlockSpec(memory_space=pl.ANY)
    return pl.pallas_call(
        functools.partial(kernel, plan),
        out_shape=jax.ShapeDtypeStruct((length, block), BF16),
        in_specs=[hbm] * 7 + [pl.BlockSpec(memory_space=pltpu.SMEM)] + [hbm] * 5,
        out_specs=pl.BlockSpec(memory_space=pltpu.VMEM),
        scratch_shapes=scratch,
        compiler_params=pltpu.CompilerParams(
            collective_id=0, has_side_effects=True, vmem_limit_bytes=67043328
        ),
        name="layer",
    )(
        seq_rows, gains, cosine, sine, query_weight, key_weight, value_weight, decay_logs, mixer_out_weight,
        value_up_weight, gate_up_weight, conv, down_weight,
    )


def solution(mesh):
    placed = (
        P("fs", "tp"), P("tp"), P("fs", "tp"), P("fs", "tp"), P("fs", "tp"), P("tp"), P("tp", "fs"), P("tp"),
        P("fs", "tp"), P("fs", "tp"), P(None, "tp"), P("tp"), P("tp", "fs"),
    )
    return jax.shard_map(
        on_device, mesh=mesh, in_specs=placed, out_specs=P("fs", "tp"), check_vma=False
    )
```

```python
import functools

import jax
import jax.numpy as jnp
import numpy as np
from jax import lax
from jax.experimental import pallas as pl
from jax.experimental.pallas import tpu as pltpu
from jax.sharding import PartitionSpec as P

DK = 256
DV = 512
KW = 3
EPS = 1e-06
ROPE_BASE = 10000.0
LANES = 128
ROWS = 256
PAD = 8
BF16 = jnp.bfloat16
F32 = jnp.float32


def flip(index, mask):
    return index + mask * (1 - 2 * lax.rem(lax.div(index, mask), 2))


def flips(index, mask):
    bit = 1
    while bit <= mask:
        if mask & bit:
            index = flip(index, bit)
        bit *= 2
    return index


def bits_of(size):
    return [1 << i for i in range(size.bit_length() - 1)]


class Plan:
    def __init__(self, fs, tp, length, block, heads_here, ff_here, shard):
        self.fs, self.tp, self.length, self.block, self.shard = fs, tp, length, block, shard
        self.width = fs * shard
        self.paired = heads_here % 2 == 0 and ff_here % LANES == 0 and fs >= 4
        self.heads = heads_here // 2 if self.paired else heads_here
        self.ff = -(-ff_here // (2 * LANES)) * LANES if self.paired else ff_here
        self.ff_step = ff_here - self.ff
        self.seqs = 2 if self.paired else 1
        self.rows = self.seqs * length
        self.pair = 2 if self.paired else 0
        bits = ([self.pair] if self.paired else []) + [b for b in bits_of(fs) if b > 1 and b != self.pair]
        self.near = 1
        self.far = []
        for bit in bits:
            self.far += [bit] + [c | bit for c in self.far]
        self.dims = [("tp", b) for b in bits_of(tp)] + ([("fs", self.pair)] if self.paired else [])
        self.qk = self.heads * DK
        self.dv = self.heads * DV
        self.heads_step = self.heads


class Mail:
    def __init__(self, sends, recvs, me):
        self.sends, self.recvs, self.me = sends, recvs, me
        self.count = 0
        self.ids = {}
        self.sent = []

    def id_of(self, key):
        if key not in self.ids:
            self.ids[key] = len(self.ids)
        return self.ids[key]

    def copy(self, key, src, dst, axis, mask):
        n = self.id_of(key)
        return pltpu.make_async_remote_copy(
            src_ref=src,
            dst_ref=dst,
            send_sem=self.sends.at[n],
            recv_sem=self.recvs.at[n],
            device_id={axis: flips(self.me[axis], mask)},
            device_id_type=pl.DeviceIdType.MESH,
        )

    def send(self, key, src, dst, axis, mask):
        copy = self.copy(key, src, dst, axis, mask)
        copy.start()
        self.sent.append((key, copy))
        return copy

    def arrive(self, key, slot, axis, mask):
        with jax.named_scope("wait_" + "_".join(str(k) for k in key)):
            self.copy(key, slot, slot, axis, mask).wait_recv()

    def drain(self, prefix):
        for key, copy in self.sent:
            if key[0].startswith(prefix):
                copy.wait_send()
        self.sent = [(key, copy) for key, copy in self.sent if not key[0].startswith(prefix)]


class Stream:
    def __init__(self, plan, mail, name, slot, stage):
        self.plan, self.mail, self.name, self.slot, self.stage = plan, mail, name, slot, stage
        self.mine = mail.me["fs"]
        self.far = list(plan.far)
        self.todo = [0] + list(plan.far)
        self.last = [c | plan.near for c in self.todo]
        self.turn = {True: 0, False: 0}

    def at(self, code):
        return self.slot(flips(self.mine, code))

    def send(self, times=1, who=None):
        for _ in range(times):
            for outer in (True, False) if who is None else (who == "outer",):
                self.turn[outer] += 1
            if who is None:
                if self.turn[True] <= len(self.far):
                    self.copy_of(self.far[self.turn[True] - 1]).start()
                continue
            turn = self.turn[who == "outer"]
            if turn > len(self.far):
                continue
            copy = self.copy_of(self.far[turn - 1])

            @pl.when(self.mail.outer if who == "outer" else jnp.logical_not(self.mail.outer))
            def _():
                copy.start()

    def copy_of(self, code):
        key = (self.name, code)
        src = self.stage if code & self.plan.pair else self.at(0)
        copy = self.mail.copy(key, src, self.at(0), "fs", code)
        if not any(k == key for k, _ in self.mail.sent):
            self.mail.sent.append((key, copy))
        return copy

    def cross(self, times=1):
        for _ in range(times):
            if self.todo:
                code = self.todo.pop(0)
                if code:
                    self.mail.arrive((self.name, code), self.at(code), "fs", code)
                self.mail.send((self.name, "x", code), self.at(code), self.at(code), "fs", self.plan.near)

    def finish(self):
        for who in ("outer", "inner"):
            self.send(max(0, len(self.far) - self.turn[who == "outer"]), who)
        self.cross(len(self.todo))
        for code in self.last:
            self.mail.arrive((self.name, "x", code & ~self.plan.near), self.at(code), "fs", self.plan.near)


def kernel(
    plan,
    x_hbm, gain_hbm, cos_hbm, sin_hbm, q_hbm, k_hbm, v_hbm, decay, out_hbm, val_hbm, gate_hbm, conv_hbm, down_hbm,
    result,
    w_in, w_out, w_val, w_gate, w_down, s_in, s_out, s_val, s_gate, s_down,
    act, act2, gains, cosine, sine, conv_par, qk, value, normed, part, hidden, gates, tail,
    *rest,
):
    n_dims = len(plan.dims)
    recvs, outs = rest[:n_dims], rest[n_dims : 2 * n_dims - 1]
    sends, arrivals, local = rest[2 * n_dims - 1 :]
    me = {"fs": lax.axis_index("fs"), "tp": lax.axis_index("tp")}
    length, block, shard = plan.length, plan.block, plan.shard
    row_blocks = length // ROWS
    seq = lax.rem(lax.div(me["fs"], plan.pair), 2) if plan.paired else 0

    barrier = pltpu.get_barrier_semaphore()
    near = [("fs", b) for b in plan.far + [plan.near]] + [d for d in plan.dims if d[0] == "tp"]
    for axis, bit in near:
        pl.semaphore_signal(
            barrier, inc=1, device_id={axis: flips(me[axis], bit)}, device_id_type=pl.DeviceIdType.MESH
        )

    places = []

    def fetch(src, dst):
        copy = pltpu.make_async_copy(src, dst, local.at[len(places)])
        copy.start()
        places.append(copy)

    def columns(index, width, size=None):
        return pl.ds(pl.multiple_of(index * width, width), size or width)

    def own_block(ref, s, t):
        return ref.at[columns(s, length), columns(t, block)]

    fetch(x_hbm, own_block(act, seq, me["tp"]))
    fetch(gain_hbm, gains.at[:, columns(me["tp"], block)])
    mine = me["fs"]
    rows_in = columns(mine, shard)

    def halves(dst, stage, take):
        fetch(take(seq), dst)
        if plan.paired:
            fetch(take(1 - seq), stage)

    qk_w, dv_w = plan.qk, plan.dv
    halves(w_in.at[rows_in, 0:qk_w], s_in.at[:, 0:qk_w], lambda h: q_hbm.at[:, columns(h, qk_w)])
    halves(
        w_in.at[rows_in, qk_w : 2 * qk_w], s_in.at[:, qk_w : 2 * qk_w], lambda h: k_hbm.at[:, columns(h, qk_w)]
    )
    halves(
        w_in.at[rows_in, 2 * qk_w : 2 * qk_w + dv_w],
        s_in.at[:, 2 * qk_w : 2 * qk_w + dv_w],
        lambda h: v_hbm.at[:, columns(h, dv_w)],
    )
    n_first = len(places)
    halves(w_out.at[:, columns(mine, shard)], s_out, lambda h: out_hbm.at[columns(h, dv_w), :])

    def ff_part(h):
        if not plan.paired:
            return slice(None)
        return pl.ds(pl.multiple_of(h * plan.ff_step, LANES), plan.ff)

    halves(w_val.at[rows_in, :], s_val, lambda h: val_hbm.at[:, ff_part(h)])
    halves(w_gate.at[rows_in, :], s_gate, lambda h: gate_hbm.at[:, ff_part(h)])
    halves(w_down.at[:, columns(mine, shard)], s_down, lambda h: down_hbm.at[ff_part(h), :])
    fetch(cos_hbm, cosine)
    fetch(sin_hbm, sine)
    fetch(conv_hbm.at[:, ff_part(seq)], conv_par)

    mail = Mail(sends, arrivals, me)
    top = plan.fs // 2
    mail.outer = lax.rem(lax.div(me["fs"], 2), 2) == lax.rem(lax.div(me["fs"], top), 2)
    st_in = Stream(plan, mail, "in", lambda j: w_in.at[columns(j, shard), :], s_in)
    st_out = Stream(plan, mail, "out", lambda j: w_out.at[:, columns(j, shard)], s_out)
    st_val = Stream(plan, mail, "val", lambda j: w_val.at[columns(j, shard), :], s_val)
    st_gate = Stream(plan, mail, "gate", lambda j: w_gate.at[columns(j, shard), :], s_gate)
    st_down = Stream(plan, mail, "down", lambda j: w_down.at[:, columns(j, shard)], s_down)

    def seq_of(dims, code):
        for place, (axis, _) in enumerate(dims):
            if axis == "fs" and code >> place & 1:
                return 1 - seq
        return seq

    def tp_of(dims, code):
        return flips(me["tp"], sum(bit for k, (axis, bit) in enumerate(dims) if axis == "tp" and code >> k & 1))

    def low(code):
        return next(i for i in range(n_dims) if code >> i & 1) if code else n_dims

    class Gather:
        def __init__(self, name, at, dims):
            self.name, self.at, self.dims = name, at, dims
            self.todo = []
            codes = [0]
            for place in range(len(self.dims) - 1, -1, -1):
                new = [c | (1 << place) for c in codes]
                self.todo += [(c, place) for c in new]
                codes = codes + new

        def forward(self, code, last):
            for place in range(last - 1, -1, -1):
                axis, bit = self.dims[place]
                mail.send((self.name, place, code), self.at(code), self.at(code), axis, bit)

        def begin(self):
            self.forward(0, len(self.dims))

        def step(self, times):
            for _ in range(times):
                if self.todo:
                    code, place = self.todo.pop(0)
                    axis, bit = self.dims[place]
                    mail.arrive((self.name, place, code & ~(1 << place)), self.at(code), axis, bit)
                    self.forward(code, place)

        def finish(self):
            self.step(len(self.todo))

    def block_rows(s, i):
        return pl.ds(pl.multiple_of(s * length + i * ROWS, ROWS), ROWS)

    class Scatter:
        def __init__(self, name, i, dims):
            self.name, self.i, self.dims = name, i, dims
            self.rows = slice(i * ROWS, (i + 1) * ROWS)
            self.waited = set()

        def multiply(self, left, right):
            def body(n, _):
                rows = block_rows(lax.div(n, plan.tp), self.i)
                cols = columns(lax.rem(n, plan.tp), block)
                part[rows, cols] = jnp.dot(left[rows, :], right[:, cols], preferred_element_type=F32).astype(BF16)
                return 0

            with jax.named_scope(f"multiply_{self.name}"):
                lax.fori_loop(0, plan.seqs * plan.tp, body, 0)
            for code in range((1 << n_dims) - 1, 0, -2):
                self.ship(code, part.at[self.term(code)])

        def term(self, code):
            return block_rows(seq_of(self.dims, code), self.i), columns(tp_of(self.dims, code), block)

        def slot(self, place, code):
            return recvs[place].at[code >> (place + 1), self.rows]

        def ship(self, code, src):
            place = low(code)
            axis, bit = self.dims[place]
            mail.send((self.name, place, code), src, self.slot(place, code), axis, bit)

        def summed(self, code):
            for k in range(low(code)):
                axis, bit = self.dims[k]
                mail.arrive((self.name, k, code | (1 << k)), self.slot(k, code), axis, bit)
            with jax.named_scope(f"sum_{self.name}_{code}"):
                total = part[self.term(code)].astype(F32)
                for k in range(low(code)):
                    total = total + recvs[k][code >> (k + 1), self.rows].astype(F32)
            return total

        def stage(self, place):
            for code in [c for c in range(1 << n_dims) if low(c) == place][::-1]:
                outs[place - 1][code >> (place + 1), self.rows] = self.summed(code).astype(BF16)
                self.ship(code, outs[place - 1].at[code >> (place + 1), self.rows])

    tp_dims = [d for d in plan.dims if d[0] == "tp"]
    gather_gain = Gather("gain", lambda c: gains.at[:, columns(tp_of(tp_dims, c), block)], tp_dims)
    gather_one = Gather(
        "one", lambda c: own_block(act, seq_of(plan.dims, c), tp_of(plan.dims, c)), plan.dims
    )

    def gather_two(i):
        def at(c):
            return act2.at[block_rows(seq_of(plan.dims, c), i), columns(tp_of(plan.dims, c), block)]

        return Gather(f"two{i}", at, plan.dims)

    for copy in places[:n_first]:
        copy.wait()
    with jax.named_scope("barrier"):
        pl.semaphore_wait(barrier, len(near))
    st_in.send(1)
    st_in.cross(1)
    gather_one.begin()
    st_in.send(2)
    gather_gain.begin()
    for copy in places[n_first:]:
        copy.wait()
    st_out.cross(1)
    st_val.cross(1)
    st_in.cross(2)
    gather_one.step(1)
    st_in.cross(1)
    st_out.send(3)
    gather_one.step(2)
    gather_gain.step(1)
    st_out.cross(1)
    st_val.send(3)
    st_out.cross(1)
    gather_one.finish()
    gather_gain.finish()
    st_in.finish()

    def scaled_rows(ref, start, gain_row):
        rows_f = ref[pl.ds(start, ROWS), :].astype(F32)
        factor = lax.rsqrt(jnp.mean(rows_f * rows_f, axis=-1, keepdims=True) + EPS)
        gain = gains[gain_row : gain_row + 1, :].astype(F32)
        return (rows_f * gain).astype(BF16), factor

    def project(i, _):
        start = pl.multiple_of(i * ROWS, ROWS)
        spot = pl.ds(pl.multiple_of(lax.rem(i, row_blocks) * ROWS, ROWS), ROWS)
        scaled, factor = scaled_rows(act, start, 0)
        total = jnp.dot(scaled, w_in[...], preferred_element_type=F32)
        cos, sin = cosine[spot, :], sine[spot, :]
        half = DK // 2
        for which, scale in ((0, 1.0), (1, DK**-0.5)):
            for head in range(plan.heads):
                at = which * qk_w + head * DK
                turned = (total[:, at : at + DK] * factor).astype(BF16).astype(F32)
                one, two = turned[:, :half], turned[:, half:]
                qk[pl.ds(start, ROWS), at : at + half] = ((one * cos - two * sin) * scale).astype(BF16)
                qk[pl.ds(start, ROWS), at + half : at + DK] = ((one * sin + two * cos) * scale).astype(BF16)
        value[pl.ds(start, ROWS), :] = (total[:, 2 * qk_w :] * factor).astype(BF16)
        return 0

    for s in range(plan.seqs):
        with jax.named_scope("project"):
            lax.fori_loop(s * row_blocks, (s + 1) * row_blocks, project, 0)
        st_out.cross(1)

    def retain(s, _):
        for head in range(plan.heads):
            log_decay = decay[seq * plan.heads + head]
            for b in range(row_blocks):
                seen = (b + 1) * ROWS
                first = pl.multiple_of(s * length, ROWS)
                rows = pl.ds(pl.multiple_of(first + b * ROWS, ROWS), ROWS)
                keys = pl.ds(first, seen)
                query = qk[rows, head * DK : (head + 1) * DK]
                key = qk[keys, qk_w + head * DK : qk_w + (head + 1) * DK]
                scores = lax.dot_general(query, key, (((1,), (1,)), ((), ())), preferred_element_type=F32)
                spread = (
                    lax.broadcasted_iota(jnp.int32, (ROWS, seen), 0)
                    - lax.broadcasted_iota(jnp.int32, (ROWS, seen), 1)
                    + b * ROWS
                )
                fall = jnp.exp(log_decay * jnp.maximum(spread, 0).astype(F32))
                scores = jnp.where(spread >= 0, scores * fall, 0.0).astype(BF16)
                ret = jnp.dot(scores, value[keys, head * DV : (head + 1) * DV], preferred_element_type=F32)
                centred = ret - jnp.mean(ret, axis=-1, keepdims=True)
                scale = lax.rsqrt(jnp.mean(centred * centred, axis=-1, keepdims=True) + EPS)
                normed[rows, head * DV : (head + 1) * DV] = (centred * scale).astype(BF16)
        return 0

    with jax.named_scope("retain"):
        lax.fori_loop(0, plan.seqs, retain, 0)
    st_gate.send(3, "inner")
    st_out.finish()

    chunks = range(row_blocks)
    own_cols = columns(me["tp"], block)
    first_sums = [Scatter(f"mixed{i}", i, plan.dims) for i in chunks]
    gathers = [gather_two(i) for i in chunks]

    def middle(i):
        mine_rows = block_rows(seq, i)
        act2[mine_rows, own_cols] = (act[mine_rows, own_cols].astype(F32) + first_sums[i].summed(0)).astype(BF16)
        gathers[i].begin()

    def stages(sums, which):
        for i in which:
            for place in range(2, n_dims):
                sums[i].stage(place)

    for i in chunks:
        first_sums[i].multiply(normed, w_out)
        first_sums[i].stage(1)
    st_val.cross(1)
    stages(first_sums, [0])
    stages(first_sums, [1])
    st_val.cross(1)
    stages(first_sums, list(chunks)[2:])
    st_gate.send(2, "outer")
    st_val.cross(1)
    middle(0)
    st_gate.cross(1)
    st_down.cross(1)
    middle(1)
    for i in chunks[2:]:
        middle(i)
    st_gate.send(1, "outer")
    st_down.send(3)
    gathers[0].step(1)
    st_gate.cross(1)
    for i in chunks[1:]:
        gathers[i].step(1)
    st_gate.cross(1)
    gathers[0].step(2)
    gathers[1].step(2)
    st_gate.cross(1)
    gathers[2].step(2)
    st_down.cross(1)
    st_val.finish()
    st_gate.finish()

    column = lax.broadcasted_iota(jnp.int32, (1, plan.ff), 1)
    keep = column >= seq * (plan.ff - plan.ff_step) if plan.paired else None

    def expand(i):
        def body(s, _):
            start = pl.multiple_of(s * length + i * ROWS, ROWS)
            scaled, factor = scaled_rows(act2, start, 1)
            gate = (jnp.dot(scaled, w_gate[...], preferred_element_type=F32) * factor).astype(BF16).astype(F32)
            if i:
                gates[0:PAD, :] = tail[s]
            else:
                gates[0:PAD, :] = jnp.zeros((PAD, plan.ff), F32)
            gates[PAD : PAD + ROWS, :] = gate
            tail[s] = gates[ROWS : ROWS + PAD, :]
            conv = conv_par[KW : KW + 1, :] + jnp.zeros((ROWS, plan.ff), F32)
            for tap in range(KW):
                at = PAD - KW + 1 + tap
                conv = conv + conv_par[tap : tap + 1, :] * gates[at : at + ROWS, :]
            up = (jnp.dot(scaled, w_val[...], preferred_element_type=F32) * factor).astype(BF16).astype(F32)
            made = conv / (1.0 + jnp.exp(-conv)) * up
            if keep is not None:
                made = jnp.where(keep, made, 0.0)
            hidden[pl.ds(start, ROWS), :] = made.astype(BF16)
            return 0

        with jax.named_scope("expand"):
            lax.fori_loop(0, plan.seqs, body, 0)

    for i in chunks:
        gathers[i].finish()
        expand(i)
        st_down.cross(1)
    st_down.finish()
    mail.drain("mixed")

    turned_dims = plan.dims[:1] + plan.dims[1:][::-1]
    last_sums = [Scatter(f"channel{i}", i, turned_dims if i % 2 else plan.dims) for i in chunks]

    def finish_rows(i):
        total = act2[block_rows(seq, i), own_cols].astype(F32) + last_sums[i].summed(0)
        result[last_sums[i].rows, :] = total.astype(BF16)

    for i in chunks:
        last_sums[i].multiply(hidden, w_down)
        last_sums[i].stage(1)
    for i in chunks:
        stages(last_sums, [i])
        if i:
            finish_rows(i - 1)
    finish_rows(row_blocks - 1)
    mail.drain("")


def on_device(
    seq_rows, mixer_gain, query_weight, key_weight, value_weight, decay_logs, mixer_out_weight, channel_gain,
    value_up_weight, gate_up_weight, conv_taps, conv_bias, down_weight,
):
    length, block = seq_rows.shape
    plan = Plan(
        lax.axis_size("fs"), lax.axis_size("tp"), length, block,
        query_weight.shape[1] // DK, value_up_weight.shape[1], query_weight.shape[0],
    )
    gains = jnp.concatenate(
        [mixer_gain[None], channel_gain[None], jnp.zeros((14, block), BF16)], axis=0
    )
    conv = jnp.concatenate(
        [conv_taps, conv_bias[None], jnp.zeros((PAD - KW - 1, conv_bias.shape[0]), BF16)], axis=0
    ).astype(F32)
    freqs = np.power(np.float32(ROPE_BASE), -np.arange(DK // 2, dtype=np.float32) * np.float32(2.0) / np.float32(DK))
    angles = np.arange(length, dtype=np.float32)[:, None] * freqs[None, :].astype(np.float32)
    cosine = jnp.asarray(np.cos(angles).astype(np.float32))
    sine = jnp.asarray(np.sin(angles).astype(np.float32))
    n_dims = len(plan.dims)
    rows, ff, width, shard = plan.rows, plan.ff, plan.width, plan.shard
    made = 2 * plan.qk + plan.dv
    vm = pltpu.VMEM
    n_mail = 5 * plan.fs + ((1 << n_dims) - 1) * (1 + 3 * (length // ROWS)) + plan.tp
    scratch = [
        vm((width, made), BF16), vm((plan.dv, width), BF16), vm((width, ff), BF16), vm((width, ff), BF16),
        vm((ff, width), BF16),
        vm((shard, made), BF16), vm((plan.dv, shard), BF16), vm((shard, ff), BF16), vm((shard, ff), BF16),
        vm((ff, shard), BF16),
        vm((rows, width), BF16), vm((rows, width), BF16), vm((16, width), BF16),
        vm((length, DK // 2), F32), vm((length, DK // 2), F32), vm((PAD, ff), F32),
        vm((rows, 2 * plan.qk), BF16), vm((rows, plan.dv), BF16), vm((rows, plan.dv), BF16),
        vm((rows, width), BF16), vm((rows, ff), BF16), vm((ROWS + PAD, ff), F32), vm((plan.seqs, PAD, ff), F32),
    ]
    scratch += [vm((1 << (n_dims - 1 - k), length, block), BF16) for k in range(n_dims)]
    scratch += [vm((1 << (n_dims - 1 - k), length, block), BF16) for k in range(1, n_dims)]
    scratch += [
        pltpu.SemaphoreType.DMA((n_mail,)), pltpu.SemaphoreType.DMA((n_mail,)), pltpu.SemaphoreType.DMA((24,)),
    ]
    hbm = pl.BlockSpec(memory_space=pl.ANY)
    return pl.pallas_call(
        functools.partial(kernel, plan),
        out_shape=jax.ShapeDtypeStruct((length, block), BF16),
        in_specs=[hbm] * 7 + [pl.BlockSpec(memory_space=pltpu.SMEM)] + [hbm] * 5,
        out_specs=pl.BlockSpec(memory_space=pltpu.VMEM),
        scratch_shapes=scratch,
        compiler_params=pltpu.CompilerParams(
            collective_id=0, has_side_effects=True, vmem_limit_bytes=67043328
        ),
        name="layer",
    )(
        seq_rows, gains, cosine, sine, query_weight, key_weight, value_weight, decay_logs, mixer_out_weight,
        value_up_weight, gate_up_weight, conv, down_weight,
    )


def solution(mesh):
    placed = (
        P("fs", "tp"), P("tp"), P("fs", "tp"), P("fs", "tp"), P("fs", "tp"), P("tp"), P("tp", "fs"), P("tp"),
        P("fs", "tp"), P("fs", "tp"), P(None, "tp"), P("tp"), P("tp", "fs"),
    )
    return jax.shard_map(
        on_device, mesh=mesh, in_specs=placed, out_specs=P("fs", "tp"), check_vma=False
    )
```

```python
import functools

import jax
import jax.numpy as jnp
import numpy as np
from jax import lax
from jax.experimental import pallas as pl
from jax.experimental.pallas import tpu as pltpu
from jax.sharding import PartitionSpec as P

DK = 256
DV = 512
KW = 3
EPS = 1e-06
ROPE_BASE = 10000.0
LANES = 128
ROWS = 256
PAD = 8
LAST_CUTS = 4
SCHEDULE = (
    ("gi", 3), "gc", "dc", "of", "m0", "m1", "vc", "m2", "s0", "s1", "vc", "s2", ("go", 2), "vc", "d0", "gc", "d1", "d2", ("go", 1), ("do", 3), ("di", 3), "g0", "g1", "gc", "g2", "gc", "h0", "h1", "h2", "dc", "vf", "gf", "e0", "dc", "e1", "e2",
)
BF16 = jnp.bfloat16
F32 = jnp.float32


def flip(index, mask):
    return index + mask * (1 - 2 * lax.rem(lax.div(index, mask), 2))


def flips(index, mask):
    bit = 1
    while bit <= mask:
        if mask & bit:
            index = flip(index, bit)
        bit *= 2
    return index


def bits_of(size):
    return [1 << i for i in range(size.bit_length() - 1)]


class Plan:
    def __init__(self, fs, tp, length, block, heads_here, ff_here, shard):
        self.fs, self.tp, self.length, self.block, self.shard = fs, tp, length, block, shard
        self.width = fs * shard
        self.paired = heads_here % 2 == 0 and ff_here % LANES == 0 and fs >= 4
        self.heads = heads_here // 2 if self.paired else heads_here
        self.packed = self.paired and ff_here % (2 * LANES) > 0
        units = ff_here // 2 if self.paired else ff_here
        self.even = units // LANES * LANES if self.packed else units
        self.units = units
        self.ff = self.even + LANES if self.packed else units
        self.half = units - self.even
        self.seqs = 2 if self.paired else 1
        self.rows = self.seqs * length
        self.pair = 2 if self.paired else 0
        bits = ([self.pair] if self.paired else []) + [b for b in bits_of(fs) if b > 1 and b != self.pair]
        self.near = 1
        self.far = []
        for bit in bits:
            self.far += [bit] + [c | bit for c in self.far]
        self.dims = [("tp", b) for b in bits_of(tp)] + ([("fs", self.pair)] if self.paired else [])
        self.qk = self.heads * DK
        self.dv = self.heads * DV
        self.heads_step = self.heads


class Mail:
    def __init__(self, sends, recvs, me):
        self.sends, self.recvs, self.me = sends, recvs, me
        self.count = 0
        self.ids = {}
        self.sent = []

    def id_of(self, key):
        if key not in self.ids:
            self.ids[key] = len(self.ids)
        return self.ids[key]

    def copy(self, key, src, dst, axis, mask):
        return self.copy_by(self.id_of(key), src, dst, axis, mask)

    def either(self, of_outer, of_inner):
        return of_outer + (1 - self.outer.astype(jnp.int32)) * (of_inner - of_outer)

    def copy_by(self, n, src, dst, axis, mask):
        return pltpu.make_async_remote_copy(
            src_ref=src,
            dst_ref=dst,
            send_sem=self.sends.at[n],
            recv_sem=self.recvs.at[n],
            device_id={axis: flips(self.me[axis], mask)},
            device_id_type=pl.DeviceIdType.MESH,
        )

    def send(self, key, src, dst, axis, mask):
        copy = self.copy(key, src, dst, axis, mask)
        copy.start()
        self.sent.append((key, copy))
        return copy

    def arrive(self, key, slot, axis, mask):
        with jax.named_scope("wait_" + "_".join(str(k) for k in key)):
            self.copy(key, slot, slot, axis, mask).wait_recv()

    def drain(self, prefix):
        for key, copy in self.sent:
            if key[0].startswith(prefix):
                copy.wait_send()
        self.sent = [(key, copy) for key, copy in self.sent if not key[0].startswith(prefix)]


class Stream:
    def __init__(self, plan, mail, name, parts, slot, stage):
        self.plan, self.mail, self.name, self.slot, self.stage, self.parts = plan, mail, name, slot, stage, parts
        self.mine = mail.me["fs"]
        self.far = list(plan.far)
        self.order = [0] + list(plan.far)
        self.order_inner = self.order[:1] + self.order[-1:] + self.order[1:-1] if plan.paired and name in ("gate", "down") else self.order
        self.crossed = self.landed = 0
        self.turn = {True: 0, False: 0}

    def at(self, code, part):
        return self.slot(flips(self.mine, code), part)

    def send(self, times=1, who=None):
        for _ in range(times):
            for outer in (True, False) if who is None else (who == "outer",):
                self.turn[outer] += 1
            if who is None:
                if self.turn[True] <= len(self.far):
                    for copy in self.copies_of(self.far[self.turn[True] - 1]):
                        copy.start()
                continue
            turn = self.turn[who == "outer"]
            if turn > len(self.far):
                continue
            copies = self.copies_of(self.far[turn - 1])

            @pl.when(self.mail.outer if who == "outer" else jnp.logical_not(self.mail.outer))
            def _():
                for copy in copies:
                    copy.start()

    def copies_of(self, code):
        copies = []
        for part in range(self.parts):
            key = (self.name, part, code)
            src = self.stage(part) if code & self.plan.pair else self.at(0, part)
            copy = self.mail.copy(key, src, self.at(0, part), "fs", code)
            copies.append(copy)
            if not any(k == key for k, _ in self.mail.sent):
                self.mail.sent.append((key, copy))
        return copies

    def code_at(self, place):
        return self.order[place], self.order_inner[place]

    def owner(self, place):
        return self.mail.either(*(flips(self.mine, code) for code in self.code_at(place)))

    def id_at(self, place, part, near):
        keys = [(self.name, part, "x", c) if near else (self.name, part, c) for c in self.code_at(place)]
        return self.mail.either(*(self.mail.id_of(key) for key in keys))

    def cross(self, times=1):
        near = self.plan.near
        for _ in range(times):
            if self.crossed == len(self.order):
                return
            place = self.crossed
            self.crossed += 1
            for part in range(self.parts):
                block = self.slot(self.owner(place), part)
                if place:
                    with jax.named_scope(f"wait_{self.name}_{part}_{place}"):
                        self.mail.copy_by(self.id_at(place, part, False), block, block, "fs", near).wait_recv()
                self.mail.copy_by(self.id_at(place, part, True), block, block, "fs", near).start()
                code = self.order[place]
                key = (self.name, part, "x", code)
                block = self.at(code, part)
                self.mail.sent.append((key, self.mail.copy(key, block, block, "fs", near)))

    def land(self, place):
        near = self.plan.near
        self.landed = place + 1
        for part in range(self.parts):
            block = self.slot(flips(self.owner(place), near), part)
            with jax.named_scope(f"wait_{self.name}_{part}_x{place}"):
                self.mail.copy_by(self.id_at(place, part, True), block, block, "fs", near).wait_recv()

    def finish(self):
        for who in ("outer", "inner"):
            self.send(max(0, len(self.far) - self.turn[who == "outer"]), who)
        self.cross(len(self.order) - self.crossed)
        for place in range(self.landed, len(self.order)):
            self.land(place)


def kernel(
    plan,
    x_hbm, gain_hbm, cos_hbm, sin_hbm, q_hbm, k_hbm, v_hbm, decay, out_hbm, val_hbm, gate_hbm, conv_hbm, down_hbm,
    result,
    w_in, w_out, w_val, w_gate, w_down, s_in, s_out, s_val, s_gate, s_down,
    act, act2, gains, cosine, sine, conv_par, qk, value, normed, part, hidden, gates, tail, tiles,
    *rest,
):
    n_dims = len(plan.dims)
    recvs, outs = rest[:n_dims], rest[n_dims : 2 * n_dims - 1]
    sends, arrivals, local = rest[2 * n_dims - 1 :]
    me = {"fs": lax.axis_index("fs"), "tp": lax.axis_index("tp")}
    length, block, shard = plan.length, plan.block, plan.shard
    row_blocks = length // ROWS
    seq = lax.rem(lax.div(me["fs"], plan.pair), 2) if plan.paired else 0

    barrier = pltpu.get_barrier_semaphore()
    near = [("fs", b) for b in plan.far + [plan.near]] + [d for d in plan.dims if d[0] == "tp"]
    for axis, bit in near:
        pl.semaphore_signal(
            barrier, inc=1, device_id={axis: flips(me[axis], bit)}, device_id_type=pl.DeviceIdType.MESH
        )

    places = []

    def fetch(src, dst):
        copy = pltpu.make_async_copy(src, dst, local.at[len(places)])
        copy.start()
        places.append(copy)

    def columns(index, width, size=None):
        return pl.ds(pl.multiple_of(index * width, width), size or width)

    def own_block(ref, s, t):
        return ref.at[columns(s, length), columns(t, block)]

    fetch(x_hbm, own_block(act, seq, me["tp"]))
    fetch(gain_hbm, gains.at[:, columns(me["tp"], block)])
    mine = me["fs"]
    rows_in = columns(mine, shard)

    def halves(dst, stage, take):
        fetch(take(seq), dst)
        if plan.paired:
            fetch(take(1 - seq), stage)

    qk_w, dv_w = plan.qk, plan.dv
    halves(w_in.at[rows_in, 0:qk_w], s_in.at[:, 0:qk_w], lambda h: q_hbm.at[:, columns(h, qk_w)])
    halves(
        w_in.at[rows_in, qk_w : 2 * qk_w], s_in.at[:, qk_w : 2 * qk_w], lambda h: k_hbm.at[:, columns(h, qk_w)]
    )
    halves(
        w_in.at[rows_in, 2 * qk_w : 2 * qk_w + dv_w],
        s_in.at[:, 2 * qk_w : 2 * qk_w + dv_w],
        lambda h: v_hbm.at[:, columns(h, dv_w)],
    )
    n_first = len(places)
    halves(w_out.at[:, columns(mine, shard)], s_out, lambda h: out_hbm.at[columns(h, dv_w), :])

    even, half = plan.even, plan.half

    def ff_part(h):
        if not plan.paired:
            return slice(None)
        return pl.ds(pl.multiple_of(h * (plan.units + half), LANES), even)

    halves(w_val.at[rows_in, :], s_val, lambda h: val_hbm.at[:, ff_part(h)])
    halves(w_gate.at[rows_in, 0:even], s_gate.at[:, 0:even], lambda h: gate_hbm.at[:, ff_part(h)])
    own_down = columns(mine, shard)
    halves(w_down.at[0:even, own_down], s_down.at[0:even, :], lambda h: down_hbm.at[ff_part(h), :])
    fetch(conv_hbm.at[:, ff_part(seq)], conv_par.at[:, 0:even])
    if plan.packed:
        middle_tile = slice(even, even + LANES)
        halves(
            w_down.at[even : even + half, own_down],
            s_down.at[even : even + half, :],
            lambda h: down_hbm.at[pl.ds(pl.multiple_of(even + h * half, half), half), :],
        )
        fetch(conv_hbm.at[:, middle_tile], conv_par.at[:, middle_tile])
        fetch(val_hbm.at[:, middle_tile], tiles.at[0])
        fetch(gate_hbm.at[:, middle_tile], tiles.at[1])
    fetch(cos_hbm, cosine)
    fetch(sin_hbm, sine)

    def swap(tile):
        return pltpu.roll(tile, half, 1)

    def pack():
        lower = lax.broadcasted_iota(jnp.int32, (1, LANES), 1) < half
        val, gate, conv = tiles[0].astype(F32), tiles[1].astype(F32), conv_par[:, middle_tile]
        first = jnp.where(lower, val, swap(gate))
        second = jnp.where(lower, swap(val), gate)
        w_gate[rows_in, middle_tile] = jnp.where(seq == 0, first, second).astype(BF16)
        s_gate[:, middle_tile] = jnp.where(seq == 0, second, first).astype(BF16)
        conv_par[:, middle_tile] = jnp.where(seq == 0, conv, swap(conv))
        w_down[even + half : even + LANES, :] = jnp.zeros((LANES - half, plan.width), BF16)

    mail = Mail(sends, arrivals, me)
    top = plan.fs // 2
    mail.outer = lax.rem(lax.div(me["fs"], 2), 2) == lax.rem(lax.div(me["fs"], top), 2)
    def cut(size, n, part):
        return slice(part * size // n, (part + 1) * size // n)

    def rows_of(ref, j, n, part):
        size = shard // n
        return ref.at[pl.ds(pl.multiple_of(j * shard + part * size, size), size), :]

    def cols_of(ref, j, rows):
        return ref.at[rows, columns(j, shard)]

    edges = (0, 2 * qk_w, 2 * qk_w + dv_w)
    st_in = Stream(
        plan, mail, "in", 2,
        lambda j, p: w_in.at[columns(j, shard), edges[p] : edges[p + 1]], lambda p: s_in.at[:, edges[p] : edges[p + 1]],
    )
    st_out = Stream(
        plan, mail, "out", 2,
        lambda j, p: cols_of(w_out, j, cut(dv_w, 2, p)), lambda p: s_out.at[cut(dv_w, 2, p), :],
    )
    st_val = Stream(
        plan, mail, "val", 2, lambda j, p: rows_of(w_val, j, 2, p), lambda p: s_val.at[cut(shard, 2, p), :]
    )
    st_gate = Stream(
        plan, mail, "gate", 2, lambda j, p: rows_of(w_gate, j, 2, p), lambda p: s_gate.at[cut(shard, 2, p), :]
    )
    st_down = Stream(
        plan, mail, "down", 2,
        lambda j, p: cols_of(w_down, j, cut(plan.units, 2, p)), lambda p: s_down.at[cut(plan.units, 2, p), :],
    )

    def seq_of(dims, code):
        for place, (axis, _) in enumerate(dims):
            if axis == "fs" and code >> place & 1:
                return 1 - seq
        return seq

    def tp_of(dims, code):
        return flips(me["tp"], sum(bit for k, (axis, bit) in enumerate(dims) if axis == "tp" and code >> k & 1))

    def low(code):
        return next(i for i in range(n_dims) if code >> i & 1) if code else n_dims

    class Gather:
        def __init__(self, name, at, dims):
            self.name, self.at, self.dims = name, at, dims
            self.todo = []
            codes = [0]
            for place in range(len(self.dims) - 1, -1, -1):
                new = [c | (1 << place) for c in codes]
                self.todo += [(c, place) for c in new]
                codes = codes + new

        def forward(self, code, last):
            for place in range(last - 1, -1, -1):
                axis, bit = self.dims[place]
                mail.send((self.name, place, code), self.at(code), self.at(code), axis, bit)

        def begin(self):
            self.forward(0, len(self.dims))

        def step(self, times):
            for _ in range(times):
                if self.todo:
                    code, place = self.todo.pop(0)
                    axis, bit = self.dims[place]
                    mail.arrive((self.name, place, code & ~(1 << place)), self.at(code), axis, bit)
                    self.forward(code, place)

        def finish(self):
            self.step(len(self.todo))

    def block_rows(s, i, size=ROWS):
        return pl.ds(pl.multiple_of(s * length + i * size, size), size)

    class Scatter:
        def __init__(self, name, i, dims, size=ROWS):
            self.name, self.i, self.dims, self.size = name, i, dims, size
            self.rows = slice(i * size, (i + 1) * size)

        def multiply(self, left, right):
            def body(n, _):
                rows = block_rows(lax.div(n, plan.tp), self.i, self.size)
                cols = columns(lax.rem(n, plan.tp), block)
                part[rows, cols] = jnp.dot(left[rows, :], right[:, cols], preferred_element_type=F32).astype(BF16)
                return 0

            with jax.named_scope(f"multiply_{self.name}"):
                lax.fori_loop(0, plan.seqs * plan.tp, body, 0)
            self.ship_first()

        def ship_first(self):
            for code in range((1 << n_dims) - 1, 0, -2):
                self.ship(code, part.at[self.term(code)])

        def term(self, code):
            return block_rows(seq_of(self.dims, code), self.i, self.size), columns(tp_of(self.dims, code), block)

        def slot(self, place, code):
            return recvs[place].at[code >> (place + 1), self.rows]

        def ship(self, code, src):
            place = low(code)
            axis, bit = self.dims[place]
            mail.send((self.name, place, code), src, self.slot(place, code), axis, bit)

        def summed(self, code):
            for k in range(low(code)):
                axis, bit = self.dims[k]
                mail.arrive((self.name, k, code | (1 << k)), self.slot(k, code), axis, bit)
            with jax.named_scope(f"sum_{self.name}_{code}"):
                total = part[self.term(code)].astype(F32)
                for k in range(low(code)):
                    total = total + recvs[k][code >> (k + 1), self.rows].astype(F32)
            return total

        def stage(self, place):
            for code in [c for c in range(1 << n_dims) if low(c) == place][::-1]:
                outs[place - 1][code >> (place + 1), self.rows] = self.summed(code).astype(BF16)
                self.ship(code, outs[place - 1].at[code >> (place + 1), self.rows])

    tp_dims = [d for d in plan.dims if d[0] == "tp"]
    gather_gain = Gather("gain", lambda c: gains.at[:, columns(tp_of(tp_dims, c), block)], tp_dims)
    gather_one = Gather(
        "one", lambda c: own_block(act, seq_of(plan.dims, c), tp_of(plan.dims, c)), plan.dims
    )

    def gather_two(i):
        def at(c):
            return act2.at[block_rows(seq_of(plan.dims, c), i), columns(tp_of(plan.dims, c), block)]

        return Gather(f"two{i}", at, plan.dims)

    for copy in places[:n_first]:
        copy.wait()
    with jax.named_scope("barrier"):
        pl.semaphore_wait(barrier, len(near))
    st_in.send(1)
    st_in.cross(1)
    gather_one.begin()
    st_in.send(2)
    gather_gain.begin()
    for copy in places[n_first:]:
        copy.wait()
    if plan.packed:
        pack()
    st_out.cross(1)
    st_val.cross(1)
    st_in.cross(2)
    gather_one.step(1)
    st_in.cross(1)
    st_out.send(3)
    gather_one.step(2)
    gather_gain.step(1)
    st_out.cross(1)
    st_val.send(3)
    st_out.cross(1)
    gather_one.finish()
    gather_gain.finish()
    st_in.finish()

    def scaled_rows(ref, start, gain_row):
        rows_f = ref[pl.ds(start, ROWS), :].astype(F32)
        factor = lax.rsqrt(jnp.mean(rows_f * rows_f, axis=-1, keepdims=True) + EPS)
        gain = gains[gain_row : gain_row + 1, :].astype(F32)
        return (rows_f * gain).astype(BF16), factor

    def project(i, _):
        start = pl.multiple_of(i * ROWS, ROWS)
        spot = pl.ds(pl.multiple_of(lax.rem(i, row_blocks) * ROWS, ROWS), ROWS)
        scaled, factor = scaled_rows(act, start, 0)
        total = jnp.dot(scaled, w_in[...], preferred_element_type=F32)
        cos, sin = cosine[spot, :], sine[spot, :]
        half = DK // 2
        for which, scale in ((0, 1.0), (1, DK**-0.5)):
            for head in range(plan.heads):
                at = which * qk_w + head * DK
                turned = (total[:, at : at + DK] * factor).astype(BF16).astype(F32)
                one, two = turned[:, :half], turned[:, half:]
                qk[pl.ds(start, ROWS), at : at + half] = ((one * cos - two * sin) * scale).astype(BF16)
                qk[pl.ds(start, ROWS), at + half : at + DK] = ((one * sin + two * cos) * scale).astype(BF16)
        value[pl.ds(start, ROWS), :] = (total[:, 2 * qk_w :] * factor).astype(BF16)
        return 0

    for s in range(plan.seqs):
        with jax.named_scope("project"):
            lax.fori_loop(s * row_blocks, (s + 1) * row_blocks, project, 0)
        st_out.cross(1)

    def retain(s, _):
        for head in range(plan.heads):
            log_decay = decay[seq * plan.heads + head]
            for b in range(row_blocks):
                seen = (b + 1) * ROWS
                first = pl.multiple_of(s * length, ROWS)
                rows = pl.ds(pl.multiple_of(first + b * ROWS, ROWS), ROWS)
                keys = pl.ds(first, seen)
                query = qk[rows, head * DK : (head + 1) * DK]
                key = qk[keys, qk_w + head * DK : qk_w + (head + 1) * DK]
                scores = lax.dot_general(query, key, (((1,), (1,)), ((), ())), preferred_element_type=F32)
                spread = (
                    lax.broadcasted_iota(jnp.int32, (ROWS, seen), 0)
                    - lax.broadcasted_iota(jnp.int32, (ROWS, seen), 1)
                    + b * ROWS
                )
                fall = jnp.exp(log_decay * jnp.maximum(spread, 0).astype(F32))
                scores = jnp.where(spread >= 0, scores * fall, 0.0).astype(BF16)
                ret = jnp.dot(scores, value[keys, head * DV : (head + 1) * DV], preferred_element_type=F32)
                centred = ret - jnp.mean(ret, axis=-1, keepdims=True)
                scale = lax.rsqrt(jnp.mean(centred * centred, axis=-1, keepdims=True) + EPS)
                normed[rows, head * DV : (head + 1) * DV] = (centred * scale).astype(BF16)
        return 0

    with jax.named_scope("retain"):
        lax.fori_loop(0, plan.seqs, retain, 0)

    chunks = range(row_blocks)
    own_cols = columns(me["tp"], block)
    first_sums = [Scatter(f"mixed{i}", i, plan.dims) for i in chunks]
    gathers = [gather_two(i) for i in chunks]

    def middle(i):
        mine_rows = block_rows(seq, i)
        act2[mine_rows, own_cols] = (act[mine_rows, own_cols].astype(F32) + first_sums[i].summed(0)).astype(BF16)
        gathers[i].begin()

    def stages(sums, which):
        for i in which:
            for place in range(2, n_dims):
                sums[i].stage(place)

    def expand(i):
        def body(s, _):
            start = pl.multiple_of(s * length + i * ROWS, ROWS)
            scaled, factor = scaled_rows(act2, start, 1)
            both = (jnp.dot(scaled, w_gate[...], preferred_element_type=F32) * factor).astype(BF16).astype(F32)
            if i:
                gates[0:PAD, :] = tail[s]
            else:
                gates[0:PAD, :] = jnp.zeros((PAD, plan.ff), F32)
            gates[PAD : PAD + ROWS, 0:even] = both[:, 0:even]
            if plan.packed:
                gates[PAD : PAD + ROWS, middle_tile] = swap(both[:, middle_tile])
            tail[s] = gates[ROWS : ROWS + PAD, :]
            conv = conv_par[KW : KW + 1, :] + jnp.zeros((ROWS, plan.ff), F32)
            for tap in range(KW):
                at = PAD - KW + 1 + tap
                conv = conv + conv_par[tap : tap + 1, :] * gates[at : at + ROWS, :]
            up = (jnp.dot(scaled, w_val[...], preferred_element_type=F32) * factor).astype(BF16).astype(F32)
            opened = conv / (1.0 + jnp.exp(-conv))
            hidden[pl.ds(start, ROWS), 0:even] = (opened[:, 0:even] * up).astype(BF16)
            if plan.packed:
                lower = lax.broadcasted_iota(jnp.int32, (1, LANES), 1) < half
                made = jnp.where(lower, opened[:, middle_tile] * both[:, middle_tile], 0.0)
                hidden[pl.ds(start, ROWS), middle_tile] = made.astype(BF16)
            return 0

        with jax.named_scope("expand"):
            lax.fori_loop(0, plan.seqs, body, 0)

    def first_terms(i):
        first_sums[i].multiply(normed, w_out)
        first_sums[i].stage(1)

    def last_gather(i):
        gathers[i].finish()
        expand(i)

    chunk_steps = {
        "m": first_terms,
        "s": lambda i: stages(first_sums, [i]),
        "d": middle,
        "g": lambda i: gathers[i].step(1),
        "h": lambda i: gathers[i].step(2),
        "e": last_gather,
    }
    streams = {"o": st_out, "v": st_val, "g": st_gate, "d": st_down}
    pending = {letter: list(chunks) for letter in chunk_steps}

    def run(letter, i):
        for before in chunk_steps:
            upto = i if before == letter else i + 1
            while pending[before] and pending[before][0] < upto:
                chunk_steps[before](pending[before].pop(0))
            if before == letter:
                break
        if i in pending[letter]:
            pending[letter].remove(i)
            chunk_steps[letter](i)

    for step in SCHEDULE:
        step, times = (step, 1) if isinstance(step, str) else step
        if step[1].isdigit():
            if int(step[1]) < row_blocks:
                run(step[0], int(step[1]))
        elif step[1] == "c":
            streams[step[0]].cross(times)
        elif step[1] == "f":
            streams[step[0]].finish()
        else:
            streams[step[0]].send(times, "outer" if step[1] == "o" else "inner")
    run("e", row_blocks - 1)
    mail.drain("mixed")

    turned_dims = plan.dims[:1] + plan.dims[1:][::-1]
    cuts = LAST_CUTS if length % (LAST_CUTS * 16) == 0 else row_blocks
    size = length // cuts
    last_sums = [Scatter(f"channel{i}", i, turned_dims if i % 2 else plan.dims, size) for i in range(cuts)]

    def reduce_columns(place, first, count, step):
        cols = columns(lax.div(st_down.owner(place), 2), 2 * shard)

        def body(n, _):
            rows = pl.ds(pl.multiple_of(first + n * step, size), size)
            part[rows, cols] = jnp.dot(hidden[rows, :], w_down[:, cols], preferred_element_type=F32).astype(BF16)
            return 0

        with jax.named_scope(f"reduce_{place}"):
            lax.fori_loop(0, count, body, 0)

    last = len(st_down.order) - 1
    for place in range(last):
        st_down.cross(max(0, place + 3 - st_down.crossed))
        st_down.land(place)
        reduce_columns(place, 0, plan.seqs * cuts, size)
    st_down.finish()

    def finish_rows(i):
        total = act2[block_rows(seq, i, size), own_cols].astype(F32) + last_sums[i].summed(0)
        result[last_sums[i].rows, :] = total.astype(BF16)

    for i in range(cuts):
        reduce_columns(last, i * size, plan.seqs, length)
        last_sums[i].ship_first()
        last_sums[i].stage(1)
        if i >= 2:
            stages(last_sums, [i - 2])
    stages(last_sums, range(max(cuts - 2, 0), cuts))
    for i in range(cuts):
        finish_rows(i)
    mail.drain("")


def on_device(
    seq_rows, mixer_gain, query_weight, key_weight, value_weight, decay_logs, mixer_out_weight, channel_gain,
    value_up_weight, gate_up_weight, conv_taps, conv_bias, down_weight,
):
    length, block = seq_rows.shape
    plan = Plan(
        lax.axis_size("fs"), lax.axis_size("tp"), length, block,
        query_weight.shape[1] // DK, value_up_weight.shape[1], query_weight.shape[0],
    )
    gains = jnp.concatenate(
        [mixer_gain[None], channel_gain[None], jnp.zeros((14, block), BF16)], axis=0
    )
    conv = jnp.concatenate(
        [conv_taps, conv_bias[None], jnp.zeros((PAD - KW - 1, conv_bias.shape[0]), BF16)], axis=0
    ).astype(F32)
    freqs = np.power(np.float32(ROPE_BASE), -np.arange(DK // 2, dtype=np.float32) * np.float32(2.0) / np.float32(DK))
    angles = np.arange(length, dtype=np.float32)[:, None] * freqs[None, :].astype(np.float32)
    cosine = jnp.asarray(np.cos(angles).astype(np.float32))
    sine = jnp.asarray(np.sin(angles).astype(np.float32))
    n_dims = len(plan.dims)
    rows, ff, width, shard = plan.rows, plan.ff, plan.width, plan.shard
    made = 2 * plan.qk + plan.dv
    vm = pltpu.VMEM
    n_mail = 10 * plan.fs + ((1 << n_dims) - 1) * (1 + 2 * (length // ROWS) + LAST_CUTS) + plan.tp
    scratch = [
        vm((width, made), BF16), vm((plan.dv, width), BF16), vm((width, plan.even), BF16), vm((width, ff), BF16),
        vm((ff, width), BF16),
        vm((shard, made), BF16), vm((plan.dv, shard), BF16), vm((shard, plan.even), BF16), vm((shard, ff), BF16),
        vm((plan.units, shard), BF16),
        vm((rows, width), BF16), vm((rows, width), BF16), vm((16, width), BF16),
        vm((length, DK // 2), F32), vm((length, DK // 2), F32), vm((PAD, ff), F32),
        vm((rows, 2 * plan.qk), BF16), vm((rows, plan.dv), BF16), vm((rows, plan.dv), BF16),
        vm((rows, width), BF16), vm((rows, ff), BF16), vm((ROWS + PAD, ff), F32), vm((plan.seqs, PAD, ff), F32),
        vm((2, shard, LANES), BF16),
    ]
    scratch += [vm((1 << (n_dims - 1 - k), length, block), BF16) for k in range(n_dims)]
    scratch += [vm((1 << (n_dims - 1 - k), length, block), BF16) for k in range(1, n_dims)]
    scratch += [
        pltpu.SemaphoreType.DMA((n_mail,)), pltpu.SemaphoreType.DMA((n_mail,)), pltpu.SemaphoreType.DMA((32,)),
    ]
    hbm = pl.BlockSpec(memory_space=pl.ANY)
    return pl.pallas_call(
        functools.partial(kernel, plan),
        out_shape=jax.ShapeDtypeStruct((length, block), BF16),
        in_specs=[hbm] * 7 + [pl.BlockSpec(memory_space=pltpu.SMEM)] + [hbm] * 5,
        out_specs=pl.BlockSpec(memory_space=pltpu.VMEM),
        scratch_shapes=scratch,
        compiler_params=pltpu.CompilerParams(
            collective_id=0, has_side_effects=True, vmem_limit_bytes=67043328
        ),
        name="layer",
    )(
        seq_rows, gains, cosine, sine, query_weight, key_weight, value_weight, decay_logs, mixer_out_weight,
        value_up_weight, gate_up_weight, conv, down_weight,
    )


def solution(mesh):
    placed = (
        P("fs", "tp"), P("tp"), P("fs", "tp"), P("fs", "tp"), P("fs", "tp"), P("tp"), P("tp", "fs"), P("tp"),
        P("fs", "tp"), P("fs", "tp"), P(None, "tp"), P("tp"), P("tp", "fs"),
    )
    return jax.shard_map(
        on_device, mesh=mesh, in_specs=placed, out_specs=P("fs", "tp"), check_vma=False
    )
```

```python
import functools

import jax
import jax.numpy as jnp
import numpy as np
from jax import lax
from jax.experimental import pallas as pl
from jax.experimental.pallas import tpu as pltpu
from jax.sharding import PartitionSpec as P

DK = 256
DV = 512
KW = 3
EPS = 1e-06
ROPE_BASE = 10000.0
LANES = 128
ROWS = 256
PAD = 8
LAST_CUTS = 4
SCHEDULE = (
    ("gi", 3), "gc", "dc", "of", "m0", "m1", "vc", "m2", "s0", "s1", "vc", "s2", ("go", 1), "vc", "d0", "gc", "d1", "d2", ("go", 2), ("do", 3), ("di", 3), "g0", "g1", "gc", "g2", "gc", "h0", "h1", "h2", "dc", "vf", "gf", "e0", "dc", "e1", "e2",
)
BF16 = jnp.bfloat16
F32 = jnp.float32


def flip(index, mask):
    return index + mask * (1 - 2 * lax.rem(lax.div(index, mask), 2))


def flips(index, mask):
    bit = 1
    while bit <= mask:
        if mask & bit:
            index = flip(index, bit)
        bit *= 2
    return index


def bits_of(size):
    return [1 << i for i in range(size.bit_length() - 1)]


class Plan:
    def __init__(self, fs, tp, length, block, heads_here, ff_here, shard):
        self.fs, self.tp, self.length, self.block, self.shard = fs, tp, length, block, shard
        self.width = fs * shard
        self.paired = heads_here % 2 == 0 and ff_here % LANES == 0 and fs >= 4
        self.heads = heads_here // 2 if self.paired else heads_here
        self.packed = self.paired and ff_here % (2 * LANES) > 0
        units = ff_here // 2 if self.paired else ff_here
        self.even = units // LANES * LANES if self.packed else units
        self.units = units
        self.ff = self.even + LANES if self.packed else units
        self.half = units - self.even
        self.seqs = 2 if self.paired else 1
        self.rows = self.seqs * length
        self.pair = 2 if self.paired else 0
        bits = ([self.pair] if self.paired else []) + [b for b in bits_of(fs) if b > 1 and b != self.pair]
        self.near = 1
        self.far = []
        for bit in bits:
            self.far += [bit] + [c | bit for c in self.far]
        self.dims = [("tp", b) for b in bits_of(tp)] + ([("fs", self.pair)] if self.paired else [])
        self.qk = self.heads * DK
        self.dv = self.heads * DV
        self.heads_step = self.heads


class Mail:
    def __init__(self, sends, recvs, me):
        self.sends, self.recvs, self.me = sends, recvs, me
        self.count = 0
        self.ids = {}
        self.sent = []

    def id_of(self, key):
        if key not in self.ids:
            self.ids[key] = len(self.ids)
        return self.ids[key]

    def copy(self, key, src, dst, axis, mask):
        return self.copy_by(self.id_of(key), src, dst, axis, mask)

    def either(self, of_outer, of_inner):
        return of_outer + (1 - self.outer.astype(jnp.int32)) * (of_inner - of_outer)

    def copy_by(self, n, src, dst, axis, mask):
        return pltpu.make_async_remote_copy(
            src_ref=src,
            dst_ref=dst,
            send_sem=self.sends.at[n],
            recv_sem=self.recvs.at[n],
            device_id={axis: flips(self.me[axis], mask)},
            device_id_type=pl.DeviceIdType.MESH,
        )

    def send(self, key, src, dst, axis, mask):
        copy = self.copy(key, src, dst, axis, mask)
        copy.start()
        self.sent.append((key, copy))
        return copy

    def arrive(self, key, slot, axis, mask):
        with jax.named_scope("wait_" + "_".join(str(k) for k in key)):
            self.copy(key, slot, slot, axis, mask).wait_recv()

    def drain(self, prefix):
        for key, copy in self.sent:
            if key[0].startswith(prefix):
                copy.wait_send()
        self.sent = [(key, copy) for key, copy in self.sent if not key[0].startswith(prefix)]


class Stream:
    def __init__(self, plan, mail, name, parts, slot, stage):
        self.plan, self.mail, self.name, self.slot, self.stage, self.parts = plan, mail, name, slot, stage, parts
        self.mine = mail.me["fs"]
        self.far = list(plan.far)
        self.order = [0] + list(plan.far)
        self.order_inner = self.order[:1] + self.order[-1:] + self.order[1:-1] if plan.paired and name in ("gate", "down") else self.order
        self.crossed = self.landed = 0
        self.turn = {True: 0, False: 0}

    def at(self, code, part):
        return self.slot(flips(self.mine, code), part)

    def send(self, times=1, who=None):
        for _ in range(times):
            for outer in (True, False) if who is None else (who == "outer",):
                self.turn[outer] += 1
            if who is None:
                if self.turn[True] <= len(self.far):
                    for copy in self.copies_of(self.far[self.turn[True] - 1]):
                        copy.start()
                continue
            turn = self.turn[who == "outer"]
            if turn > len(self.far):
                continue
            copies = self.copies_of(self.far[turn - 1])

            @pl.when(self.mail.outer if who == "outer" else jnp.logical_not(self.mail.outer))
            def _():
                for copy in copies:
                    copy.start()

    def copies_of(self, code):
        copies = []
        for part in range(self.parts):
            key = (self.name, part, code)
            src = self.stage(part) if code & self.plan.pair else self.at(0, part)
            copy = self.mail.copy(key, src, self.at(0, part), "fs", code)
            copies.append(copy)
            if not any(k == key for k, _ in self.mail.sent):
                self.mail.sent.append((key, copy))
        return copies

    def code_at(self, place):
        return self.order[place], self.order_inner[place]

    def owner(self, place):
        return self.mail.either(*(flips(self.mine, code) for code in self.code_at(place)))

    def id_at(self, place, part, near):
        keys = [(self.name, part, "x", c) if near else (self.name, part, c) for c in self.code_at(place)]
        return self.mail.either(*(self.mail.id_of(key) for key in keys))

    def cross(self, times=1):
        near = self.plan.near
        for _ in range(times):
            if self.crossed == len(self.order):
                return
            place = self.crossed
            self.crossed += 1
            for part in range(self.parts):
                block = self.slot(self.owner(place), part)
                if place:
                    with jax.named_scope(f"wait_{self.name}_{part}_{place}"):
                        self.mail.copy_by(self.id_at(place, part, False), block, block, "fs", near).wait_recv()
                self.mail.copy_by(self.id_at(place, part, True), block, block, "fs", near).start()
                code = self.order[place]
                key = (self.name, part, "x", code)
                block = self.at(code, part)
                self.mail.sent.append((key, self.mail.copy(key, block, block, "fs", near)))

    def land(self, place):
        near = self.plan.near
        self.landed = place + 1
        for part in range(self.parts):
            block = self.slot(flips(self.owner(place), near), part)
            with jax.named_scope(f"wait_{self.name}_{part}_x{place}"):
                self.mail.copy_by(self.id_at(place, part, True), block, block, "fs", near).wait_recv()

    def finish(self):
        for who in ("outer", "inner"):
            self.send(max(0, len(self.far) - self.turn[who == "outer"]), who)
        self.cross(len(self.order) - self.crossed)
        for place in range(self.landed, len(self.order)):
            self.land(place)


def kernel(
    plan,
    x_hbm, gain_hbm, cos_hbm, sin_hbm, q_hbm, k_hbm, v_hbm, decay, out_hbm, val_hbm, gate_hbm, conv_hbm, down_hbm,
    result,
    w_in, w_out, w_val, w_gate, w_down, s_in, s_out, s_val, s_gate, s_down,
    act, act2, gains, cosine, sine, conv_par, qk, value, normed, part, hidden, gates, tail, tiles,
    *rest,
):
    n_dims = len(plan.dims)
    recvs, outs = rest[:n_dims], rest[n_dims : 2 * n_dims - 1]
    sends, arrivals, local = rest[2 * n_dims - 1 :]
    me = {"fs": lax.axis_index("fs"), "tp": lax.axis_index("tp")}
    length, block, shard = plan.length, plan.block, plan.shard
    row_blocks = length // ROWS
    seq = lax.rem(lax.div(me["fs"], plan.pair), 2) if plan.paired else 0

    barrier = pltpu.get_barrier_semaphore()
    near = [("fs", b) for b in plan.far + [plan.near]] + [d for d in plan.dims if d[0] == "tp"]
    for axis, bit in near:
        pl.semaphore_signal(
            barrier, inc=1, device_id={axis: flips(me[axis], bit)}, device_id_type=pl.DeviceIdType.MESH
        )

    places = []

    def fetch(src, dst):
        copy = pltpu.make_async_copy(src, dst, local.at[len(places)])
        copy.start()
        places.append(copy)

    def columns(index, width, size=None):
        return pl.ds(pl.multiple_of(index * width, width), size or width)

    def own_block(ref, s, t):
        return ref.at[columns(s, length), columns(t, block)]

    fetch(x_hbm, own_block(act, seq, me["tp"]))
    fetch(gain_hbm, gains.at[:, columns(me["tp"], block)])
    mine = me["fs"]
    rows_in = columns(mine, shard)

    def halves(dst, stage, take):
        fetch(take(seq), dst)
        if plan.paired:
            fetch(take(1 - seq), stage)

    qk_w, dv_w = plan.qk, plan.dv
    halves(w_in.at[rows_in, 0:qk_w], s_in.at[:, 0:qk_w], lambda h: q_hbm.at[:, columns(h, qk_w)])
    halves(
        w_in.at[rows_in, qk_w : 2 * qk_w], s_in.at[:, qk_w : 2 * qk_w], lambda h: k_hbm.at[:, columns(h, qk_w)]
    )
    halves(
        w_in.at[rows_in, 2 * qk_w : 2 * qk_w + dv_w],
        s_in.at[:, 2 * qk_w : 2 * qk_w + dv_w],
        lambda h: v_hbm.at[:, columns(h, dv_w)],
    )
    n_first = len(places)
    halves(w_out.at[:, columns(mine, shard)], s_out, lambda h: out_hbm.at[columns(h, dv_w), :])

    even, half = plan.even, plan.half

    def ff_part(h):
        if not plan.paired:
            return slice(None)
        return pl.ds(pl.multiple_of(h * (plan.units + half), LANES), even)

    halves(w_val.at[rows_in, :], s_val, lambda h: val_hbm.at[:, ff_part(h)])
    halves(w_gate.at[rows_in, 0:even], s_gate.at[:, 0:even], lambda h: gate_hbm.at[:, ff_part(h)])
    own_down = columns(mine, shard)
    halves(w_down.at[0:even, own_down], s_down.at[0:even, :], lambda h: down_hbm.at[ff_part(h), :])
    fetch(conv_hbm.at[:, ff_part(seq)], conv_par.at[:, 0:even])
    if plan.packed:
        middle_tile = slice(even, even + LANES)
        halves(
            w_down.at[even : even + half, own_down],
            s_down.at[even : even + half, :],
            lambda h: down_hbm.at[pl.ds(pl.multiple_of(even + h * half, half), half), :],
        )
        fetch(conv_hbm.at[:, middle_tile], conv_par.at[:, middle_tile])
        fetch(val_hbm.at[:, middle_tile], tiles.at[0])
        fetch(gate_hbm.at[:, middle_tile], tiles.at[1])
    fetch(cos_hbm, cosine)
    fetch(sin_hbm, sine)

    def swap(tile):
        return pltpu.roll(tile, half, 1)

    def pack():
        lower = lax.broadcasted_iota(jnp.int32, (1, LANES), 1) < half
        val, gate, conv = tiles[0].astype(F32), tiles[1].astype(F32), conv_par[:, middle_tile]
        first = jnp.where(lower, val, swap(gate))
        second = jnp.where(lower, swap(val), gate)
        w_gate[rows_in, middle_tile] = jnp.where(seq == 0, first, second).astype(BF16)
        s_gate[:, middle_tile] = jnp.where(seq == 0, second, first).astype(BF16)
        conv_par[:, middle_tile] = jnp.where(seq == 0, conv, swap(conv))
        w_down[even + half : even + LANES, :] = jnp.zeros((LANES - half, plan.width), BF16)

    mail = Mail(sends, arrivals, me)
    top = plan.fs // 2
    mail.outer = lax.rem(lax.div(me["fs"], 2), 2) == lax.rem(lax.div(me["fs"], top), 2)
    def cut(size, n, part):
        return slice(part * size // n, (part + 1) * size // n)

    def rows_of(ref, j, n, part):
        size = shard // n
        return ref.at[pl.ds(pl.multiple_of(j * shard + part * size, size), size), :]

    def cols_of(ref, j, rows):
        return ref.at[rows, columns(j, shard)]

    edges = (0, 2 * qk_w, 2 * qk_w + dv_w)
    st_in = Stream(
        plan, mail, "in", 2,
        lambda j, p: w_in.at[columns(j, shard), edges[p] : edges[p + 1]], lambda p: s_in.at[:, edges[p] : edges[p + 1]],
    )
    st_out = Stream(
        plan, mail, "out", 2,
        lambda j, p: cols_of(w_out, j, cut(dv_w, 2, p)), lambda p: s_out.at[cut(dv_w, 2, p), :],
    )
    st_val = Stream(
        plan, mail, "val", 2, lambda j, p: rows_of(w_val, j, 2, p), lambda p: s_val.at[cut(shard, 2, p), :]
    )
    st_gate = Stream(
        plan, mail, "gate", 2, lambda j, p: rows_of(w_gate, j, 2, p), lambda p: s_gate.at[cut(shard, 2, p), :]
    )
    st_down = Stream(
        plan, mail, "down", 2,
        lambda j, p: cols_of(w_down, j, cut(plan.units, 2, p)), lambda p: s_down.at[cut(plan.units, 2, p), :],
    )

    def seq_of(dims, code):
        for place, (axis, _) in enumerate(dims):
            if axis == "fs" and code >> place & 1:
                return 1 - seq
        return seq

    def tp_of(dims, code):
        return flips(me["tp"], sum(bit for k, (axis, bit) in enumerate(dims) if axis == "tp" and code >> k & 1))

    def low(code):
        return next(i for i in range(n_dims) if code >> i & 1) if code else n_dims

    class Gather:
        def __init__(self, name, at, dims):
            self.name, self.at, self.dims = name, at, dims
            self.todo = []
            codes = [0]
            for place in range(len(self.dims) - 1, -1, -1):
                new = [c | (1 << place) for c in codes]
                self.todo += [(c, place) for c in new]
                codes = codes + new

        def forward(self, code, last):
            for place in range(last - 1, -1, -1):
                axis, bit = self.dims[place]
                mail.send((self.name, place, code), self.at(code), self.at(code), axis, bit)

        def begin(self):
            self.forward(0, len(self.dims))

        def step(self, times):
            for _ in range(times):
                if self.todo:
                    code, place = self.todo.pop(0)
                    axis, bit = self.dims[place]
                    mail.arrive((self.name, place, code & ~(1 << place)), self.at(code), axis, bit)
                    self.forward(code, place)

        def finish(self):
            self.step(len(self.todo))

    def block_rows(s, i, size=ROWS):
        return pl.ds(pl.multiple_of(s * length + i * size, size), size)

    class Scatter:
        def __init__(self, name, i, dims, size=ROWS):
            self.name, self.i, self.dims, self.size = name, i, dims, size
            self.rows = slice(i * size, (i + 1) * size)

        def multiply(self, left, right):
            def body(n, _):
                rows = block_rows(lax.div(n, plan.tp), self.i, self.size)
                cols = columns(lax.rem(n, plan.tp), block)
                part[rows, cols] = jnp.dot(left[rows, :], right[:, cols], preferred_element_type=F32).astype(BF16)
                return 0

            with jax.named_scope(f"multiply_{self.name}"):
                lax.fori_loop(0, plan.seqs * plan.tp, body, 0)
            self.ship_first()

        def ship_first(self):
            for code in range((1 << n_dims) - 1, 0, -2):
                self.ship(code, part.at[self.term(code)])

        def term(self, code):
            return block_rows(seq_of(self.dims, code), self.i, self.size), columns(tp_of(self.dims, code), block)

        def slot(self, place, code):
            return recvs[place].at[code >> (place + 1), self.rows]

        def ship(self, code, src):
            place = low(code)
            axis, bit = self.dims[place]
            mail.send((self.name, place, code), src, self.slot(place, code), axis, bit)

        def summed(self, code):
            for k in range(low(code)):
                axis, bit = self.dims[k]
                mail.arrive((self.name, k, code | (1 << k)), self.slot(k, code), axis, bit)
            with jax.named_scope(f"sum_{self.name}_{code}"):
                total = part[self.term(code)].astype(F32)
                for k in range(low(code)):
                    total = total + recvs[k][code >> (k + 1), self.rows].astype(F32)
            return total

        def stage(self, place):
            for code in [c for c in range(1 << n_dims) if low(c) == place][::-1]:
                outs[place - 1][code >> (place + 1), self.rows] = self.summed(code).astype(BF16)
                self.ship(code, outs[place - 1].at[code >> (place + 1), self.rows])

    tp_dims = [d for d in plan.dims if d[0] == "tp"]
    gather_gain = Gather("gain", lambda c: gains.at[:, columns(tp_of(tp_dims, c), block)], tp_dims)
    gather_one = Gather(
        "one", lambda c: own_block(act, seq_of(plan.dims, c), tp_of(plan.dims, c)), plan.dims
    )

    def gather_two(i):
        def at(c):
            return act2.at[block_rows(seq_of(plan.dims, c), i), columns(tp_of(plan.dims, c), block)]

        return Gather(f"two{i}", at, plan.dims)

    for copy in places[:n_first]:
        copy.wait()
    with jax.named_scope("barrier"):
        pl.semaphore_wait(barrier, len(near))
    st_in.send(1)
    st_in.cross(1)
    gather_one.begin()
    st_in.send(2)
    gather_gain.begin()
    for copy in places[n_first:]:
        copy.wait()
    if plan.packed:
        pack()
    st_out.cross(1)
    st_val.cross(1)
    st_in.cross(2)
    gather_one.step(1)
    st_in.cross(1)
    st_out.send(3)
    gather_one.step(2)
    gather_gain.step(1)
    st_out.cross(1)
    st_val.send(3)
    st_out.cross(1)
    gather_one.finish()
    gather_gain.finish()
    st_in.finish()

    def scaled_rows(ref, start, gain_row):
        rows_f = ref[pl.ds(start, ROWS), :].astype(F32)
        factor = lax.rsqrt(jnp.mean(rows_f * rows_f, axis=-1, keepdims=True) + EPS)
        gain = gains[gain_row : gain_row + 1, :].astype(F32)
        return (rows_f * gain).astype(BF16), factor

    def project(i, _):
        start = pl.multiple_of(i * ROWS, ROWS)
        spot = pl.ds(pl.multiple_of(lax.rem(i, row_blocks) * ROWS, ROWS), ROWS)
        scaled, factor = scaled_rows(act, start, 0)
        total = jnp.dot(scaled, w_in[...], preferred_element_type=F32)
        cos, sin = cosine[spot, :], sine[spot, :]
        half = DK // 2
        for which, scale in ((0, 1.0), (1, DK**-0.5)):
            for head in range(plan.heads):
                at = which * qk_w + head * DK
                turned = (total[:, at : at + DK] * factor).astype(BF16).astype(F32)
                one, two = turned[:, :half], turned[:, half:]
                qk[pl.ds(start, ROWS), at : at + half] = ((one * cos - two * sin) * scale).astype(BF16)
                qk[pl.ds(start, ROWS), at + half : at + DK] = ((one * sin + two * cos) * scale).astype(BF16)
        value[pl.ds(start, ROWS), :] = (total[:, 2 * qk_w :] * factor).astype(BF16)
        return 0

    for s in range(plan.seqs):
        with jax.named_scope("project"):
            lax.fori_loop(s * row_blocks, (s + 1) * row_blocks, project, 0)
        st_out.cross(1)

    def retain(s, _):
        for head in range(plan.heads):
            log_decay = decay[seq * plan.heads + head]
            for b in range(row_blocks):
                seen = (b + 1) * ROWS
                first = pl.multiple_of(s * length, ROWS)
                rows = pl.ds(pl.multiple_of(first + b * ROWS, ROWS), ROWS)
                keys = pl.ds(first, seen)
                query = qk[rows, head * DK : (head + 1) * DK]
                key = qk[keys, qk_w + head * DK : qk_w + (head + 1) * DK]
                scores = lax.dot_general(query, key, (((1,), (1,)), ((), ())), preferred_element_type=F32)
                spread = (
                    lax.broadcasted_iota(jnp.int32, (ROWS, seen), 0)
                    - lax.broadcasted_iota(jnp.int32, (ROWS, seen), 1)
                    + b * ROWS
                )
                fall = jnp.exp(log_decay * jnp.maximum(spread, 0).astype(F32))
                scores = jnp.where(spread >= 0, scores * fall, 0.0).astype(BF16)
                ret = jnp.dot(scores, value[keys, head * DV : (head + 1) * DV], preferred_element_type=F32)
                centred = ret - jnp.mean(ret, axis=-1, keepdims=True)
                scale = lax.rsqrt(jnp.mean(centred * centred, axis=-1, keepdims=True) + EPS)
                normed[rows, head * DV : (head + 1) * DV] = (centred * scale).astype(BF16)
        return 0

    with jax.named_scope("retain"):
        lax.fori_loop(0, plan.seqs, retain, 0)

    chunks = range(row_blocks)
    own_cols = columns(me["tp"], block)
    first_sums = [Scatter(f"mixed{i}", i, plan.dims) for i in chunks]
    gathers = [gather_two(i) for i in chunks]

    def middle(i):
        mine_rows = block_rows(seq, i)
        act2[mine_rows, own_cols] = (act[mine_rows, own_cols].astype(F32) + first_sums[i].summed(0)).astype(BF16)
        gathers[i].begin()

    def stages(sums, which):
        for i in which:
            for place in range(2, n_dims):
                sums[i].stage(place)

    def expand(i):
        def body(s, _):
            start = pl.multiple_of(s * length + i * ROWS, ROWS)
            scaled, factor = scaled_rows(act2, start, 1)
            both = (jnp.dot(scaled, w_gate[...], preferred_element_type=F32) * factor).astype(BF16).astype(F32)
            if i:
                gates[0:PAD, :] = tail[s]
            else:
                gates[0:PAD, :] = jnp.zeros((PAD, plan.ff), F32)
            gates[PAD : PAD + ROWS, 0:even] = both[:, 0:even]
            if plan.packed:
                gates[PAD : PAD + ROWS, middle_tile] = swap(both[:, middle_tile])
            tail[s] = gates[ROWS : ROWS + PAD, :]
            conv = conv_par[KW : KW + 1, :] + jnp.zeros((ROWS, plan.ff), F32)
            for tap in range(KW):
                at = PAD - KW + 1 + tap
                conv = conv + conv_par[tap : tap + 1, :] * gates[at : at + ROWS, :]
            up = (jnp.dot(scaled, w_val[...], preferred_element_type=F32) * factor).astype(BF16).astype(F32)
            opened = conv / (1.0 + jnp.exp(-conv))
            hidden[pl.ds(start, ROWS), 0:even] = (opened[:, 0:even] * up).astype(BF16)
            if plan.packed:
                lower = lax.broadcasted_iota(jnp.int32, (1, LANES), 1) < half
                made = jnp.where(lower, opened[:, middle_tile] * both[:, middle_tile], 0.0)
                hidden[pl.ds(start, ROWS), middle_tile] = made.astype(BF16)
            return 0

        with jax.named_scope("expand"):
            lax.fori_loop(0, plan.seqs, body, 0)

    def first_terms(i):
        first_sums[i].multiply(normed, w_out)
        first_sums[i].stage(1)

    def last_gather(i):
        gathers[i].finish()
        expand(i)

    chunk_steps = {
        "m": first_terms,
        "s": lambda i: stages(first_sums, [i]),
        "d": middle,
        "g": lambda i: gathers[i].step(1),
        "h": lambda i: gathers[i].step(2),
        "e": last_gather,
    }
    streams = {"o": st_out, "v": st_val, "g": st_gate, "d": st_down}
    pending = {letter: list(chunks) for letter in chunk_steps}

    def run(letter, i):
        for before in chunk_steps:
            upto = i if before == letter else i + 1
            while pending[before] and pending[before][0] < upto:
                chunk_steps[before](pending[before].pop(0))
            if before == letter:
                break
        if i in pending[letter]:
            pending[letter].remove(i)
            chunk_steps[letter](i)

    for step in SCHEDULE:
        step, times = (step, 1) if isinstance(step, str) else step
        if step[1].isdigit():
            if int(step[1]) < row_blocks:
                run(step[0], int(step[1]))
        elif step[1] == "c":
            streams[step[0]].cross(times)
        elif step[1] == "f":
            streams[step[0]].finish()
        else:
            streams[step[0]].send(times, "outer" if step[1] == "o" else "inner")
    run("e", row_blocks - 1)
    mail.drain("mixed")

    turned_dims = plan.dims[:1] + plan.dims[1:][::-1]
    cuts = LAST_CUTS if length % (LAST_CUTS * 16) == 0 else row_blocks
    size = length // cuts
    last_sums = [Scatter(f"channel{i}", i, turned_dims if i % 2 else plan.dims, size) for i in range(cuts)]

    def reduce_columns(place, first, count, step):
        cols = columns(lax.div(st_down.owner(place), 2), 2 * shard)

        def body(n, _):
            rows = pl.ds(pl.multiple_of(first + n * step, size), size)
            part[rows, cols] = jnp.dot(hidden[rows, :], w_down[:, cols], preferred_element_type=F32).astype(BF16)
            return 0

        with jax.named_scope(f"reduce_{place}"):
            lax.fori_loop(0, count, body, 0)

    last = len(st_down.order) - 1
    for place in range(last):
        st_down.cross(max(0, place + 3 - st_down.crossed))
        st_down.land(place)
        reduce_columns(place, 0, plan.seqs * cuts, size)
    st_down.finish()

    def finish_rows(i):
        total = act2[block_rows(seq, i, size), own_cols].astype(F32) + last_sums[i].summed(0)
        result[last_sums[i].rows, :] = total.astype(BF16)

    for i in range(cuts):
        reduce_columns(last, i * size, plan.seqs, length)
        last_sums[i].ship_first()
        if i % 2 or i == cuts - 1:
            for k in range(i - i % 2, i + 1):
                last_sums[k].stage(1)
    for i in range(cuts):
        stages(last_sums, [i])
    for i in range(cuts):
        finish_rows(i)
    mail.drain("")


def on_device(
    seq_rows, mixer_gain, query_weight, key_weight, value_weight, decay_logs, mixer_out_weight, channel_gain,
    value_up_weight, gate_up_weight, conv_taps, conv_bias, down_weight,
):
    length, block = seq_rows.shape
    plan = Plan(
        lax.axis_size("fs"), lax.axis_size("tp"), length, block,
        query_weight.shape[1] // DK, value_up_weight.shape[1], query_weight.shape[0],
    )
    gains = jnp.concatenate(
        [mixer_gain[None], channel_gain[None], jnp.zeros((14, block), BF16)], axis=0
    )
    conv = jnp.concatenate(
        [conv_taps, conv_bias[None], jnp.zeros((PAD - KW - 1, conv_bias.shape[0]), BF16)], axis=0
    ).astype(F32)
    freqs = np.power(np.float32(ROPE_BASE), -np.arange(DK // 2, dtype=np.float32) * np.float32(2.0) / np.float32(DK))
    angles = np.arange(length, dtype=np.float32)[:, None] * freqs[None, :].astype(np.float32)
    cosine = jnp.asarray(np.cos(angles).astype(np.float32))
    sine = jnp.asarray(np.sin(angles).astype(np.float32))
    n_dims = len(plan.dims)
    rows, ff, width, shard = plan.rows, plan.ff, plan.width, plan.shard
    made = 2 * plan.qk + plan.dv
    vm = pltpu.VMEM
    n_mail = 10 * plan.fs + ((1 << n_dims) - 1) * (1 + 2 * (length // ROWS) + LAST_CUTS) + plan.tp
    scratch = [
        vm((width, made), BF16), vm((plan.dv, width), BF16), vm((width, plan.even), BF16), vm((width, ff), BF16),
        vm((ff, width), BF16),
        vm((shard, made), BF16), vm((plan.dv, shard), BF16), vm((shard, plan.even), BF16), vm((shard, ff), BF16),
        vm((plan.units, shard), BF16),
        vm((rows, width), BF16), vm((rows, width), BF16), vm((16, width), BF16),
        vm((length, DK // 2), F32), vm((length, DK // 2), F32), vm((PAD, ff), F32),
        vm((rows, 2 * plan.qk), BF16), vm((rows, plan.dv), BF16), vm((rows, plan.dv), BF16),
        vm((rows, width), BF16), vm((rows, ff), BF16), vm((ROWS + PAD, ff), F32), vm((plan.seqs, PAD, ff), F32),
        vm((2, shard, LANES), BF16),
    ]
    scratch += [vm((1 << (n_dims - 1 - k), length, block), BF16) for k in range(n_dims)]
    scratch += [vm((1 << (n_dims - 1 - k), length, block), BF16) for k in range(1, n_dims)]
    scratch += [
        pltpu.SemaphoreType.DMA((n_mail,)), pltpu.SemaphoreType.DMA((n_mail,)), pltpu.SemaphoreType.DMA((32,)),
    ]
    hbm = pl.BlockSpec(memory_space=pl.ANY)
    return pl.pallas_call(
        functools.partial(kernel, plan),
        out_shape=jax.ShapeDtypeStruct((length, block), BF16),
        in_specs=[hbm] * 7 + [pl.BlockSpec(memory_space=pltpu.SMEM)] + [hbm] * 5,
        out_specs=pl.BlockSpec(memory_space=pltpu.VMEM),
        scratch_shapes=scratch,
        compiler_params=pltpu.CompilerParams(
            collective_id=0, has_side_effects=True, vmem_limit_bytes=67043328
        ),
        name="layer",
    )(
        seq_rows, gains, cosine, sine, query_weight, key_weight, value_weight, decay_logs, mixer_out_weight,
        value_up_weight, gate_up_weight, conv, down_weight,
    )


def solution(mesh):
    placed = (
        P("fs", "tp"), P("tp"), P("fs", "tp"), P("fs", "tp"), P("fs", "tp"), P("tp"), P("tp", "fs"), P("tp"),
        P("fs", "tp"), P("fs", "tp"), P(None, "tp"), P("tp"), P("tp", "fs"),
    )
    return jax.shard_map(
        on_device, mesh=mesh, in_specs=placed, out_specs=P("fs", "tp"), check_vma=False
    )
```

```python
import functools

import jax
import jax.numpy as jnp
import numpy as np
from jax import lax
from jax.experimental import pallas as pl
from jax.experimental.pallas import tpu as pltpu
from jax.sharding import PartitionSpec as P

DK = 256
DV = 512
KW = 3
EPS = 1e-06
ROPE_BASE = 10000.0
LANES = 128
ROWS = 256
PAD = 8
LAST_CUTS = 4
SCHEDULE = (
    ("gi", 3), "gc", "dc", "of", "m0", "m1", "vc", "m2", "s0", "s1", "vc", "s2", ("go", 1), "d0", "vc", "gc", "d1", "d2", ("go", 2), ("di", 3), ("do", 3), "g0", "g1", "gc", "g2", "gc", "h0", "h1", "h2", "dc", "vf", "gf", "e0", "dc", "e1", "e2",
)
BF16 = jnp.bfloat16
F32 = jnp.float32


def flip(index, mask):
    return index + mask * (1 - 2 * lax.rem(lax.div(index, mask), 2))


def flips(index, mask):
    bit = 1
    while bit <= mask:
        if mask & bit:
            index = flip(index, bit)
        bit *= 2
    return index


def bits_of(size):
    return [1 << i for i in range(size.bit_length() - 1)]


class Plan:
    def __init__(self, fs, tp, length, block, heads_here, ff_here, shard):
        self.fs, self.tp, self.length, self.block, self.shard = fs, tp, length, block, shard
        self.width = fs * shard
        self.paired = heads_here % 2 == 0 and ff_here % LANES == 0 and fs >= 4
        self.heads = heads_here // 2 if self.paired else heads_here
        self.packed = self.paired and ff_here % (2 * LANES) > 0
        units = ff_here // 2 if self.paired else ff_here
        self.even = units // LANES * LANES if self.packed else units
        self.units = units
        self.ff = self.even + LANES if self.packed else units
        self.half = units - self.even
        self.seqs = 2 if self.paired else 1
        self.rows = self.seqs * length
        self.pair = 2 if self.paired else 0
        bits = ([self.pair] if self.paired else []) + [b for b in bits_of(fs) if b > 1 and b != self.pair]
        self.near = 1
        self.far = []
        for bit in bits:
            self.far += [bit] + [c | bit for c in self.far]
        self.dims = [("tp", b) for b in bits_of(tp)] + ([("fs", self.pair)] if self.paired else [])
        self.qk = self.heads * DK
        self.dv = self.heads * DV
        self.heads_step = self.heads


class Mail:
    def __init__(self, sends, recvs, me):
        self.sends, self.recvs, self.me = sends, recvs, me
        self.count = 0
        self.ids = {}
        self.sent = []

    def id_of(self, key):
        if key not in self.ids:
            self.ids[key] = len(self.ids)
        return self.ids[key]

    def copy(self, key, src, dst, axis, mask):
        return self.copy_by(self.id_of(key), src, dst, axis, mask)

    def either(self, of_outer, of_inner):
        return of_outer + (1 - self.outer.astype(jnp.int32)) * (of_inner - of_outer)

    def copy_by(self, n, src, dst, axis, mask):
        return pltpu.make_async_remote_copy(
            src_ref=src,
            dst_ref=dst,
            send_sem=self.sends.at[n],
            recv_sem=self.recvs.at[n],
            device_id={axis: flips(self.me[axis], mask)},
            device_id_type=pl.DeviceIdType.MESH,
        )

    def send(self, key, src, dst, axis, mask):
        copy = self.copy(key, src, dst, axis, mask)
        copy.start()
        self.sent.append((key, copy))
        return copy

    def arrive(self, key, slot, axis, mask):
        with jax.named_scope("wait_" + "_".join(str(k) for k in key)):
            self.copy(key, slot, slot, axis, mask).wait_recv()

    def drain(self, prefix):
        for key, copy in self.sent:
            if key[0].startswith(prefix):
                copy.wait_send()
        self.sent = [(key, copy) for key, copy in self.sent if not key[0].startswith(prefix)]


class Stream:
    def __init__(self, plan, mail, name, parts, slot, stage):
        self.plan, self.mail, self.name, self.slot, self.stage, self.parts = plan, mail, name, slot, stage, parts
        self.mine = mail.me["fs"]
        self.far = list(plan.far)
        self.order = [0] + list(plan.far)
        self.order_inner = self.order[:1] + self.order[-1:] + self.order[1:-1] if plan.paired and name in ("gate", "down") else self.order
        self.crossed = self.landed = 0
        self.turn = {True: 0, False: 0}

    def at(self, code, part):
        return self.slot(flips(self.mine, code), part)

    def send(self, times=1, who=None):
        for _ in range(times):
            for outer in (True, False) if who is None else (who == "outer",):
                self.turn[outer] += 1
            if who is None:
                if self.turn[True] <= len(self.far):
                    for copy in self.copies_of(self.far[self.turn[True] - 1]):
                        copy.start()
                continue
            turn = self.turn[who == "outer"]
            if turn > len(self.far):
                continue
            copies = self.copies_of(self.far[turn - 1])

            @pl.when(self.mail.outer if who == "outer" else jnp.logical_not(self.mail.outer))
            def _():
                for copy in copies:
                    copy.start()

    def copies_of(self, code):
        copies = []
        for part in range(self.parts):
            key = (self.name, part, code)
            src = self.stage(part) if code & self.plan.pair else self.at(0, part)
            copy = self.mail.copy(key, src, self.at(0, part), "fs", code)
            copies.append(copy)
            if not any(k == key for k, _ in self.mail.sent):
                self.mail.sent.append((key, copy))
        return copies

    def code_at(self, place):
        return self.order[place], self.order_inner[place]

    def owner(self, place):
        return self.mail.either(*(flips(self.mine, code) for code in self.code_at(place)))

    def id_at(self, place, part, near):
        keys = [(self.name, part, "x", c) if near else (self.name, part, c) for c in self.code_at(place)]
        return self.mail.either(*(self.mail.id_of(key) for key in keys))

    def cross(self, times=1):
        near = self.plan.near
        for _ in range(times):
            if self.crossed == len(self.order):
                return
            place = self.crossed
            self.crossed += 1
            for part in range(self.parts):
                block = self.slot(self.owner(place), part)
                if place:
                    with jax.named_scope(f"wait_{self.name}_{part}_{place}"):
                        self.mail.copy_by(self.id_at(place, part, False), block, block, "fs", near).wait_recv()
                self.mail.copy_by(self.id_at(place, part, True), block, block, "fs", near).start()
                code = self.order[place]
                key = (self.name, part, "x", code)
                block = self.at(code, part)
                self.mail.sent.append((key, self.mail.copy(key, block, block, "fs", near)))

    def land(self, place):
        near = self.plan.near
        self.landed = place + 1
        for part in range(self.parts):
            block = self.slot(flips(self.owner(place), near), part)
            with jax.named_scope(f"wait_{self.name}_{part}_x{place}"):
                self.mail.copy_by(self.id_at(place, part, True), block, block, "fs", near).wait_recv()

    def finish(self):
        for who in ("outer", "inner"):
            self.send(max(0, len(self.far) - self.turn[who == "outer"]), who)
        self.cross(len(self.order) - self.crossed)
        for place in range(self.landed, len(self.order)):
            self.land(place)


def kernel(
    plan,
    x_hbm, gain_hbm, cos_hbm, sin_hbm, q_hbm, k_hbm, v_hbm, decay, out_hbm, val_hbm, gate_hbm, conv_hbm, down_hbm,
    result,
    w_in, w_out, w_val, w_gate, w_down, s_in, s_out, s_val, s_gate, s_down,
    act, act2, gains, cosine, sine, conv_par, qk, value, normed, part, hidden, gates, tail, tiles,
    *rest,
):
    n_dims = len(plan.dims)
    recvs, outs = rest[:n_dims], rest[n_dims : 2 * n_dims - 1]
    sends, arrivals, local = rest[2 * n_dims - 1 :]
    me = {"fs": lax.axis_index("fs"), "tp": lax.axis_index("tp")}
    length, block, shard = plan.length, plan.block, plan.shard
    row_blocks = length // ROWS
    seq = lax.rem(lax.div(me["fs"], plan.pair), 2) if plan.paired else 0

    barrier = pltpu.get_barrier_semaphore()
    near = [("fs", b) for b in plan.far + [plan.near]] + [d for d in plan.dims if d[0] == "tp"]
    for axis, bit in near:
        pl.semaphore_signal(
            barrier, inc=1, device_id={axis: flips(me[axis], bit)}, device_id_type=pl.DeviceIdType.MESH
        )

    places = []

    def fetch(src, dst):
        copy = pltpu.make_async_copy(src, dst, local.at[len(places)])
        copy.start()
        places.append(copy)

    def columns(index, width, size=None):
        return pl.ds(pl.multiple_of(index * width, width), size or width)

    def own_block(ref, s, t):
        return ref.at[columns(s, length), columns(t, block)]

    fetch(x_hbm, own_block(act, seq, me["tp"]))
    fetch(gain_hbm, gains.at[:, columns(me["tp"], block)])
    mine = me["fs"]
    rows_in = columns(mine, shard)

    def halves(dst, stage, take):
        fetch(take(seq), dst)
        if plan.paired:
            fetch(take(1 - seq), stage)

    qk_w, dv_w = plan.qk, plan.dv
    halves(w_in.at[rows_in, 0:qk_w], s_in.at[:, 0:qk_w], lambda h: q_hbm.at[:, columns(h, qk_w)])
    halves(
        w_in.at[rows_in, qk_w : 2 * qk_w], s_in.at[:, qk_w : 2 * qk_w], lambda h: k_hbm.at[:, columns(h, qk_w)]
    )
    halves(
        w_in.at[rows_in, 2 * qk_w : 2 * qk_w + dv_w],
        s_in.at[:, 2 * qk_w : 2 * qk_w + dv_w],
        lambda h: v_hbm.at[:, columns(h, dv_w)],
    )
    n_first = len(places)
    halves(w_out.at[:, columns(mine, shard)], s_out, lambda h: out_hbm.at[columns(h, dv_w), :])

    even, half = plan.even, plan.half

    def ff_part(h):
        if not plan.paired:
            return slice(None)
        return pl.ds(pl.multiple_of(h * (plan.units + half), LANES), even)

    halves(w_val.at[rows_in, :], s_val, lambda h: val_hbm.at[:, ff_part(h)])
    halves(w_gate.at[rows_in, 0:even], s_gate.at[:, 0:even], lambda h: gate_hbm.at[:, ff_part(h)])
    own_down = columns(mine, shard)
    halves(w_down.at[0:even, own_down], s_down.at[0:even, :], lambda h: down_hbm.at[ff_part(h), :])
    fetch(conv_hbm.at[:, ff_part(seq)], conv_par.at[:, 0:even])
    if plan.packed:
        middle_tile = slice(even, even + LANES)
        halves(
            w_down.at[even : even + half, own_down],
            s_down.at[even : even + half, :],
            lambda h: down_hbm.at[pl.ds(pl.multiple_of(even + h * half, half), half), :],
        )
        fetch(conv_hbm.at[:, middle_tile], conv_par.at[:, middle_tile])
        fetch(val_hbm.at[:, middle_tile], tiles.at[0])
        fetch(gate_hbm.at[:, middle_tile], tiles.at[1])
    fetch(cos_hbm, cosine)
    fetch(sin_hbm, sine)

    def swap(tile):
        return pltpu.roll(tile, half, 1)

    def pack():
        lower = lax.broadcasted_iota(jnp.int32, (1, LANES), 1) < half
        val, gate, conv = tiles[0].astype(F32), tiles[1].astype(F32), conv_par[:, middle_tile]
        first = jnp.where(lower, val, swap(gate))
        second = jnp.where(lower, swap(val), gate)
        w_gate[rows_in, middle_tile] = jnp.where(seq == 0, first, second).astype(BF16)
        s_gate[:, middle_tile] = jnp.where(seq == 0, second, first).astype(BF16)
        conv_par[:, middle_tile] = jnp.where(seq == 0, conv, swap(conv))
        w_down[even + half : even + LANES, :] = jnp.zeros((LANES - half, plan.width), BF16)

    mail = Mail(sends, arrivals, me)
    top = plan.fs // 2
    mail.outer = lax.rem(lax.div(me["fs"], 2), 2) == lax.rem(lax.div(me["fs"], top), 2)
    def cut(size, n, part):
        return slice(part * size // n, (part + 1) * size // n)

    def rows_of(ref, j, n, part):
        size = shard // n
        return ref.at[pl.ds(pl.multiple_of(j * shard + part * size, size), size), :]

    def cols_of(ref, j, rows):
        return ref.at[rows, columns(j, shard)]

    edges = (0, 2 * qk_w, 2 * qk_w + dv_w)
    st_in = Stream(
        plan, mail, "in", 2,
        lambda j, p: w_in.at[columns(j, shard), edges[p] : edges[p + 1]], lambda p: s_in.at[:, edges[p] : edges[p + 1]],
    )
    st_out = Stream(
        plan, mail, "out", 2,
        lambda j, p: cols_of(w_out, j, cut(dv_w, 2, p)), lambda p: s_out.at[cut(dv_w, 2, p), :],
    )
    st_val = Stream(
        plan, mail, "val", 2, lambda j, p: rows_of(w_val, j, 2, p), lambda p: s_val.at[cut(shard, 2, p), :]
    )
    st_gate = Stream(
        plan, mail, "gate", 2, lambda j, p: rows_of(w_gate, j, 2, p), lambda p: s_gate.at[cut(shard, 2, p), :]
    )
    st_down = Stream(
        plan, mail, "down", 2,
        lambda j, p: cols_of(w_down, j, cut(plan.units, 2, p)), lambda p: s_down.at[cut(plan.units, 2, p), :],
    )

    def seq_of(dims, code):
        for place, (axis, _) in enumerate(dims):
            if axis == "fs" and code >> place & 1:
                return 1 - seq
        return seq

    def tp_of(dims, code):
        return flips(me["tp"], sum(bit for k, (axis, bit) in enumerate(dims) if axis == "tp" and code >> k & 1))

    def low(code):
        return next(i for i in range(n_dims) if code >> i & 1) if code else n_dims

    class Gather:
        def __init__(self, name, at, dims):
            self.name, self.at, self.dims = name, at, dims
            self.todo = []
            codes = [0]
            for place in range(len(self.dims) - 1, -1, -1):
                new = [c | (1 << place) for c in codes]
                self.todo += [(c, place) for c in new]
                codes = codes + new

        def forward(self, code, last):
            for place in range(last - 1, -1, -1):
                axis, bit = self.dims[place]
                mail.send((self.name, place, code), self.at(code), self.at(code), axis, bit)

        def begin(self):
            self.forward(0, len(self.dims))

        def step(self, times):
            for _ in range(times):
                if self.todo:
                    code, place = self.todo.pop(0)
                    axis, bit = self.dims[place]
                    mail.arrive((self.name, place, code & ~(1 << place)), self.at(code), axis, bit)
                    self.forward(code, place)

        def finish(self):
            self.step(len(self.todo))

    def block_rows(s, i, size=ROWS):
        return pl.ds(pl.multiple_of(s * length + i * size, size), size)

    class Scatter:
        def __init__(self, name, i, dims, size=ROWS):
            self.name, self.i, self.dims, self.size = name, i, dims, size
            self.rows = slice(i * size, (i + 1) * size)

        def multiply(self, left, right):
            def body(n, _):
                rows = block_rows(lax.div(n, plan.tp), self.i, self.size)
                cols = columns(lax.rem(n, plan.tp), block)
                part[rows, cols] = jnp.dot(left[rows, :], right[:, cols], preferred_element_type=F32).astype(BF16)
                return 0

            with jax.named_scope(f"multiply_{self.name}"):
                lax.fori_loop(0, plan.seqs * plan.tp, body, 0)
            self.ship_first()

        def ship_first(self):
            for code in range((1 << n_dims) - 1, 0, -2):
                self.ship(code, part.at[self.term(code)])

        def term(self, code):
            return block_rows(seq_of(self.dims, code), self.i, self.size), columns(tp_of(self.dims, code), block)

        def slot(self, place, code):
            return recvs[place].at[code >> (place + 1), self.rows]

        def ship(self, code, src):
            place = low(code)
            axis, bit = self.dims[place]
            mail.send((self.name, place, code), src, self.slot(place, code), axis, bit)

        def summed(self, code):
            for k in range(low(code)):
                axis, bit = self.dims[k]
                mail.arrive((self.name, k, code | (1 << k)), self.slot(k, code), axis, bit)
            with jax.named_scope(f"sum_{self.name}_{code}"):
                total = part[self.term(code)].astype(F32)
                for k in range(low(code)):
                    total = total + recvs[k][code >> (k + 1), self.rows].astype(F32)
            return total

        def stage(self, place):
            for code in [c for c in range(1 << n_dims) if low(c) == place][::-1]:
                outs[place - 1][code >> (place + 1), self.rows] = self.summed(code).astype(BF16)
                self.ship(code, outs[place - 1].at[code >> (place + 1), self.rows])

    tp_dims = [d for d in plan.dims if d[0] == "tp"]
    gather_gain = Gather("gain", lambda c: gains.at[:, columns(tp_of(tp_dims, c), block)], tp_dims)
    gather_one = Gather(
        "one", lambda c: own_block(act, seq_of(plan.dims, c), tp_of(plan.dims, c)), plan.dims
    )

    def gather_two(i):
        def at(c):
            return act2.at[block_rows(seq_of(plan.dims, c), i), columns(tp_of(plan.dims, c), block)]

        return Gather(f"two{i}", at, plan.dims)

    for copy in places[:n_first]:
        copy.wait()
    with jax.named_scope("barrier"):
        pl.semaphore_wait(barrier, len(near))
    st_in.send(1)
    st_in.cross(1)
    gather_one.begin()
    st_in.send(2)
    gather_gain.begin()
    for copy in places[n_first:]:
        copy.wait()
    if plan.packed:
        pack()
    st_out.cross(1)
    st_val.cross(1)
    st_in.cross(2)
    gather_one.step(1)
    st_in.cross(1)
    st_out.send(3)
    gather_one.step(2)
    gather_gain.step(1)
    st_out.cross(1)
    st_val.send(3)
    st_out.cross(1)
    gather_one.finish()
    gather_gain.finish()
    st_in.finish()

    def scaled_rows(ref, start, gain_row):
        rows_f = ref[pl.ds(start, ROWS), :].astype(F32)
        factor = lax.rsqrt(jnp.mean(rows_f * rows_f, axis=-1, keepdims=True) + EPS)
        gain = gains[gain_row : gain_row + 1, :].astype(F32)
        return (rows_f * gain).astype(BF16), factor

    def project(i, _):
        start = pl.multiple_of(i * ROWS, ROWS)
        spot = pl.ds(pl.multiple_of(lax.rem(i, row_blocks) * ROWS, ROWS), ROWS)
        scaled, factor = scaled_rows(act, start, 0)
        total = jnp.dot(scaled, w_in[...], preferred_element_type=F32)
        cos, sin = cosine[spot, :], sine[spot, :]
        half = DK // 2
        for which, scale in ((0, 1.0), (1, DK**-0.5)):
            for head in range(plan.heads):
                at = which * qk_w + head * DK
                turned = (total[:, at : at + DK] * factor).astype(BF16).astype(F32)
                one, two = turned[:, :half], turned[:, half:]
                qk[pl.ds(start, ROWS), at : at + half] = ((one * cos - two * sin) * scale).astype(BF16)
                qk[pl.ds(start, ROWS), at + half : at + DK] = ((one * sin + two * cos) * scale).astype(BF16)
        value[pl.ds(start, ROWS), :] = (total[:, 2 * qk_w :] * factor).astype(BF16)
        return 0

    for s in range(plan.seqs):
        with jax.named_scope("project"):
            lax.fori_loop(s * row_blocks, (s + 1) * row_blocks, project, 0)
        st_out.cross(1)

    def retain(s, _):
        for head in range(plan.heads):
            log_decay = decay[seq * plan.heads + head]
            for b in range(row_blocks):
                seen = (b + 1) * ROWS
                first = pl.multiple_of(s * length, ROWS)
                rows = pl.ds(pl.multiple_of(first + b * ROWS, ROWS), ROWS)
                keys = pl.ds(first, seen)
                query = qk[rows, head * DK : (head + 1) * DK]
                key = qk[keys, qk_w + head * DK : qk_w + (head + 1) * DK]
                scores = lax.dot_general(query, key, (((1,), (1,)), ((), ())), preferred_element_type=F32)
                spread = (
                    lax.broadcasted_iota(jnp.int32, (ROWS, seen), 0)
                    - lax.broadcasted_iota(jnp.int32, (ROWS, seen), 1)
                    + b * ROWS
                )
                fall = jnp.exp(log_decay * jnp.maximum(spread, 0).astype(F32))
                scores = jnp.where(spread >= 0, scores * fall, 0.0).astype(BF16)
                ret = jnp.dot(scores, value[keys, head * DV : (head + 1) * DV], preferred_element_type=F32)
                centred = ret - jnp.mean(ret, axis=-1, keepdims=True)
                scale = lax.rsqrt(jnp.mean(centred * centred, axis=-1, keepdims=True) + EPS)
                normed[rows, head * DV : (head + 1) * DV] = (centred * scale).astype(BF16)
        return 0

    with jax.named_scope("retain"):
        lax.fori_loop(0, plan.seqs, retain, 0)

    chunks = range(row_blocks)
    own_cols = columns(me["tp"], block)
    first_sums = [Scatter(f"mixed{i}", i, plan.dims) for i in chunks]
    gathers = [gather_two(i) for i in chunks]

    def middle(i):
        mine_rows = block_rows(seq, i)
        act2[mine_rows, own_cols] = (act[mine_rows, own_cols].astype(F32) + first_sums[i].summed(0)).astype(BF16)
        gathers[i].begin()

    def stages(sums, which):
        for i in which:
            for place in range(2, n_dims):
                sums[i].stage(place)

    def expand(i):
        def body(s, _):
            start = pl.multiple_of(s * length + i * ROWS, ROWS)
            scaled, factor = scaled_rows(act2, start, 1)
            both = (jnp.dot(scaled, w_gate[...], preferred_element_type=F32) * factor).astype(BF16).astype(F32)
            if i:
                gates[0:PAD, :] = tail[s]
            else:
                gates[0:PAD, :] = jnp.zeros((PAD, plan.ff), F32)
            gates[PAD : PAD + ROWS, 0:even] = both[:, 0:even]
            if plan.packed:
                gates[PAD : PAD + ROWS, middle_tile] = swap(both[:, middle_tile])
            tail[s] = gates[ROWS : ROWS + PAD, :]
            conv = conv_par[KW : KW + 1, :] + jnp.zeros((ROWS, plan.ff), F32)
            for tap in range(KW):
                at = PAD - KW + 1 + tap
                conv = conv + conv_par[tap : tap + 1, :] * gates[at : at + ROWS, :]
            up = (jnp.dot(scaled, w_val[...], preferred_element_type=F32) * factor).astype(BF16).astype(F32)
            opened = conv / (1.0 + jnp.exp(-conv))
            hidden[pl.ds(start, ROWS), 0:even] = (opened[:, 0:even] * up).astype(BF16)
            if plan.packed:
                lower = lax.broadcasted_iota(jnp.int32, (1, LANES), 1) < half
                made = jnp.where(lower, opened[:, middle_tile] * both[:, middle_tile], 0.0)
                hidden[pl.ds(start, ROWS), middle_tile] = made.astype(BF16)
            return 0

        with jax.named_scope("expand"):
            lax.fori_loop(0, plan.seqs, body, 0)

    def first_terms(i):
        first_sums[i].multiply(normed, w_out)
        first_sums[i].stage(1)

    def last_gather(i):
        gathers[i].finish()
        expand(i)

    chunk_steps = {
        "m": first_terms,
        "s": lambda i: stages(first_sums, [i]),
        "d": middle,
        "g": lambda i: gathers[i].step(1),
        "h": lambda i: gathers[i].step(2),
        "e": last_gather,
    }
    streams = {"o": st_out, "v": st_val, "g": st_gate, "d": st_down}
    pending = {letter: list(chunks) for letter in chunk_steps}

    def run(letter, i):
        for before in chunk_steps:
            upto = i if before == letter else i + 1
            while pending[before] and pending[before][0] < upto:
                chunk_steps[before](pending[before].pop(0))
            if before == letter:
                break
        if i in pending[letter]:
            pending[letter].remove(i)
            chunk_steps[letter](i)

    for step in SCHEDULE:
        step, times = (step, 1) if isinstance(step, str) else step
        if step[1].isdigit():
            if int(step[1]) < row_blocks:
                run(step[0], int(step[1]))
        elif step[1] == "c":
            streams[step[0]].cross(times)
        elif step[1] == "f":
            streams[step[0]].finish()
        else:
            streams[step[0]].send(times, "outer" if step[1] == "o" else "inner")
    run("e", row_blocks - 1)
    mail.drain("mixed")

    turned_dims = plan.dims[:1] + plan.dims[1:][::-1]
    cuts = LAST_CUTS if length % (LAST_CUTS * 16) == 0 else row_blocks
    size = length // cuts
    last_sums = [Scatter(f"channel{i}", i, turned_dims if i % 2 else plan.dims, size) for i in range(cuts)]

    def reduce_columns(place, first, count, step):
        cols = columns(lax.div(st_down.owner(place), 2), 2 * shard)

        def body(n, _):
            rows = pl.ds(pl.multiple_of(first + n * step, size), size)
            part[rows, cols] = jnp.dot(hidden[rows, :], w_down[:, cols], preferred_element_type=F32).astype(BF16)
            return 0

        with jax.named_scope(f"reduce_{place}"):
            lax.fori_loop(0, count, body, 0)

    last = len(st_down.order) - 1
    for place in range(last):
        st_down.cross(max(0, place + 3 - st_down.crossed))
        st_down.land(place)
        reduce_columns(place, 0, plan.seqs * cuts, size)
    st_down.finish()

    def finish_rows(i):
        total = act2[block_rows(seq, i, size), own_cols].astype(F32) + last_sums[i].summed(0)
        result[last_sums[i].rows, :] = total.astype(BF16)

    for i in range(cuts):
        reduce_columns(last, i * size, plan.seqs, length)
        last_sums[i].ship_first()
        if i % 2 or i == cuts - 1:
            for k in range(i - i % 2, i + 1):
                last_sums[k].stage(1)
    for i in range(cuts):
        stages(last_sums, [i])
    for i in range(cuts):
        finish_rows(i)
    mail.drain("")


def on_device(
    seq_rows, mixer_gain, query_weight, key_weight, value_weight, decay_logs, mixer_out_weight, channel_gain,
    value_up_weight, gate_up_weight, conv_taps, conv_bias, down_weight,
):
    length, block = seq_rows.shape
    plan = Plan(
        lax.axis_size("fs"), lax.axis_size("tp"), length, block,
        query_weight.shape[1] // DK, value_up_weight.shape[1], query_weight.shape[0],
    )
    gains = jnp.concatenate(
        [mixer_gain[None], channel_gain[None], jnp.zeros((14, block), BF16)], axis=0
    )
    conv = jnp.concatenate(
        [conv_taps, conv_bias[None], jnp.zeros((PAD - KW - 1, conv_bias.shape[0]), BF16)], axis=0
    ).astype(F32)
    freqs = np.power(np.float32(ROPE_BASE), -np.arange(DK // 2, dtype=np.float32) * np.float32(2.0) / np.float32(DK))
    angles = np.arange(length, dtype=np.float32)[:, None] * freqs[None, :].astype(np.float32)
    cosine = jnp.asarray(np.cos(angles).astype(np.float32))
    sine = jnp.asarray(np.sin(angles).astype(np.float32))
    n_dims = len(plan.dims)
    rows, ff, width, shard = plan.rows, plan.ff, plan.width, plan.shard
    made = 2 * plan.qk + plan.dv
    vm = pltpu.VMEM
    n_mail = 10 * plan.fs + ((1 << n_dims) - 1) * (1 + 2 * (length // ROWS) + LAST_CUTS) + plan.tp
    scratch = [
        vm((width, made), BF16), vm((plan.dv, width), BF16), vm((width, plan.even), BF16), vm((width, ff), BF16),
        vm((ff, width), BF16),
        vm((shard, made), BF16), vm((plan.dv, shard), BF16), vm((shard, plan.even), BF16), vm((shard, ff), BF16),
        vm((plan.units, shard), BF16),
        vm((rows, width), BF16), vm((rows, width), BF16), vm((16, width), BF16),
        vm((length, DK // 2), F32), vm((length, DK // 2), F32), vm((PAD, ff), F32),
        vm((rows, 2 * plan.qk), BF16), vm((rows, plan.dv), BF16), vm((rows, plan.dv), BF16),
        vm((rows, width), BF16), vm((rows, ff), BF16), vm((ROWS + PAD, ff), F32), vm((plan.seqs, PAD, ff), F32),
        vm((2, shard, LANES), BF16),
    ]
    scratch += [vm((1 << (n_dims - 1 - k), length, block), BF16) for k in range(n_dims)]
    scratch += [vm((1 << (n_dims - 1 - k), length, block), BF16) for k in range(1, n_dims)]
    scratch += [
        pltpu.SemaphoreType.DMA((n_mail,)), pltpu.SemaphoreType.DMA((n_mail,)), pltpu.SemaphoreType.DMA((32,)),
    ]
    hbm = pl.BlockSpec(memory_space=pl.ANY)
    return pl.pallas_call(
        functools.partial(kernel, plan),
        out_shape=jax.ShapeDtypeStruct((length, block), BF16),
        in_specs=[hbm] * 7 + [pl.BlockSpec(memory_space=pltpu.SMEM)] + [hbm] * 5,
        out_specs=pl.BlockSpec(memory_space=pltpu.VMEM),
        scratch_shapes=scratch,
        compiler_params=pltpu.CompilerParams(
            collective_id=0, has_side_effects=True, vmem_limit_bytes=67043328
        ),
        name="layer",
    )(
        seq_rows, gains, cosine, sine, query_weight, key_weight, value_weight, decay_logs, mixer_out_weight,
        value_up_weight, gate_up_weight, conv, down_weight,
    )


def solution(mesh):
    placed = (
        P("fs", "tp"), P("tp"), P("fs", "tp"), P("fs", "tp"), P("fs", "tp"), P("tp"), P("tp", "fs"), P("tp"),
        P("fs", "tp"), P("fs", "tp"), P(None, "tp"), P("tp"), P("tp", "fs"),
    )
    return jax.shard_map(
        on_device, mesh=mesh, in_specs=placed, out_specs=P("fs", "tp"), check_vma=False
    )
```
